32 devices in a mesh: ep: 8 (over z, core), tp: 4 (over y, x).
Axes of the slice: x: 2, y: 2, z: 4, core: 2. Of those that a mesh axis runs over, the one named last changes fastest.
Arguments:
- outer_gate: bfloat16 [1024, 2048], P('ep', 'tp'), may hold values from -6 to 6
- inner_gate: bfloat16 [1024, 2048], P('ep', 'tp'), may hold values from -6 to 6
- conv_value: bfloat16 [1024, 2048], P('ep', 'tp'), may hold values from -6 to 6
- conv_taps: bfloat16 [3, 2048], P(None, 'tp'), may hold values from -3.5 to 3.5
- mix_out: bfloat16 [2048, 2048], P(None, 'tp')
- gain_mixer: bfloat16 [2048], P('tp'), may hold values from 0.099609375 to 1.8984375
- bias_mixer: bfloat16 [2048], P('tp'), may hold values from -3 to 3
- moe_input: bfloat16 [1024, 2048], P('ep'), may hold values from -6 to 6
- route_ids: int32 [1024, 4], P('ep'), may hold values from 0 to 7, all different within a row; in each aligned block of 128 rows (0 to 127, 128 to 255, ...) at most 96 rows name the same one
- route_weights: float32 [1024, 4], P('ep'), may hold values from 0.1 to 1.2
- expert_gate: bfloat16 [8, 2048, 2048], P('ep', None, 'tp'), may hold values from -0.125 to 0.125
- expert_up: bfloat16 [8, 2048, 2048], P('ep', None, 'tp'), may hold values from -0.125 to 0.125
- expert_down: bfloat16 [8, 2048, 2048], P('ep', None, 'tp')
- shared_gate: bfloat16 [2048, 2048], P(None, 'tp'), may hold values from -0.125 to 0.125
- shared_up: bfloat16 [2048, 2048], P(None, 'tp'), may hold values from -0.125 to 0.125
- shared_down: bfloat16 [2048, 2048], P(None, 'tp')
- gain_experts: bfloat16 [2048], P('tp'), may hold values from 0.099609375 to 1.8984375
- bias_experts: bfloat16 [2048], P('tp'), may hold values from -3 to 3
Outputs:
- out_mixer: bfloat16 [1024, 2048], P('ep', 'tp')
- out_experts: bfloat16 [1024, 2048], P('ep', 'tp')
The draws below stay inside these ranges and needn't reach their ends.
Inputs may be any that keep to these rules, and one draw needn't show every extreme that they name: `route_ids`: each row names 4 different experts. Among the rows of one index of ep (aligned blocks of 128 rows) no expert is named more than 96 times, a bound that some block reaches.
All inputs are finite; a program needn't handle non-finite values.
Results may differ from the reference program's by a relative error of at most 0.0055.
Values may be sent and summed in bfloat16 or wider, within the bound.
A program may use at most 64 MiB of HBM per device.

```python
import math
import jax
import jax.numpy as jnp
import numpy as np
from jax import lax

D = 2048
EFF = 2048
SFF = 2048
KERNEL = 3
TOPK = 4
ROWS = 128
TOKENS = 1024
EXPERTS = 8
CAP = 96
SEQ_LEN = 1024
N_EP = 8


def column_scales(key, width):
    place = jnp.arange(width, dtype=jnp.float32) / width
    rough = jax.random.uniform(jax.random.fold_in(key, 7), (width,), jnp.float32, 0.5, 2.0)
    return jnp.exp(jnp.log(10.0) * place) * rough


def draw_mix_out(key, part):
    values = jax.random.normal(jax.random.fold_in(key, 11), (D, D), jnp.float32) * D ** (-0.5)
    return (values * column_scales(key, D)[None, :]).astype(jnp.bfloat16)


def draw_expert_down(key, part):
    values = jax.random.normal(jax.random.fold_in(key, 13), (EXPERTS, EFF, D), jnp.float32) * EFF ** (-0.5)
    return (values * column_scales(key, D)[None, None, :]).astype(jnp.bfloat16)


def draw_shared_down(key, part):
    values = jax.random.normal(jax.random.fold_in(key, 17), (SFF, D), jnp.float32) * SFF ** (-0.5)
    return (values * column_scales(key, D)[None, :]).astype(jnp.bfloat16)


def level_of(rng, shape, shards, smallest, top_value):
    factor_of, own = 1.0, jax.random.fold_in(rng, 6)
    for position, parts in shards:
        steps = jnp.exp(jax.random.uniform(jax.random.fold_in(own, position), (parts,), jnp.float32, smallest / len(shards), top_value / len(shards)))
        factor_of = factor_of * jnp.repeat(steps, shape[position] // parts).reshape([-1 if axis == position else 1 for axis in range(len(shape))])
    return factor_of


def assign_block(own_key, own, number, rows, count, top, reach, skew):
    order = jax.random.permutation(own_key, count)
    heavy_load, common = shares(count, rows * top, reach, skew, True), shares(count, rows * top, reach, skew, False)
    places = jnp.arange(count)

    def named(lengths, turn):
        used = int((lengths > 0).sum())
        fixed = max(1, used // 4)
        passed = fixed + (places - fixed + turn * (used - fixed)) % max(1, count - fixed)
        return jnp.zeros((count,), jnp.int32).at[order[jnp.where(places < fixed, places, passed)]].set(jnp.asarray(lengths, jnp.int32))

    lengths = jnp.where(number % 4 == 0, named(heavy_load, number // 4), named(common, number - number // 4 - 1))
    mixed = jax.random.permutation(jax.random.fold_in(own, 3), count)
    donor, sink = mixed[0:count // 2 * 2:2], mixed[1:count // 2 * 2:2]
    room = jnp.minimum(lengths[donor] - 1, reach - lengths[sink]) // 2
    room = jnp.where((donor == order[0]) | (sink == order[0]) | (lengths[sink] == 0), 0, jnp.maximum(room, 0))
    passed = jax.random.randint(jax.random.fold_in(own, 4), (count // 2,), 0, 1 << 20) % (room + 1)
    lengths = lengths.at[donor].add(-passed).at[sink].add(passed)
    items = jnp.searchsorted(jnp.cumsum(lengths), jnp.arange(rows * top), side="right").astype(jnp.int32)
    grid = items.reshape(top, rows).T
    grid = grid[jax.random.permutation(jax.random.fold_in(own, 1), rows)]
    turn = jax.random.randint(jax.random.fold_in(own, 2), (rows, 1), 0, top)
    return jnp.take_along_axis(grid, (jnp.arange(top)[None, :] + turn) % top, axis=1)


def shares(number_of, total, reach, slope, full):
    portions = [(1 << 20) // math.isqrt(rank ** slope) + 1 for rank in range(1, number_of + 1)]
    largest = reach if full else min(reach, max(-(-total // number_of), total * portions[0] // sum(portions)))
    least = 1 if total - largest >= number_of - 1 else 0
    given, surplus = [largest] + [least] * (number_of - 1), total - largest - least * (number_of - 1)
    while surplus > 0:
        candidates = [i for i in range(1, number_of) if given[i] < largest] or [i for i in range(1, number_of) if given[i] < reach]
        mass, budget = sum([portions[i] for i in candidates]), surplus
        for i in candidates:
            addition = min(reach - given[i], max(1, budget * portions[i] // mass), surplus)
            given[i] = given[i] + addition
            surplus = surplus - addition
    return np.array(given)


def gaussian(own_key, shape, scale, bound, cuts=(), kind=jnp.bfloat16):
    drawn = jax.random.normal(own_key, shape, jnp.float32) * scale
    if len(cuts) > 0:
        drawn = level_of(own_key, shape, cuts, -0.22, 0.18) * drawn
    return jnp.clip(drawn, min=-bound, max=bound).astype(kind)


def setup_inputs(seed: int = 0) -> dict:
    key_list = jax.random.split(jax.random.key(seed), 19)
    outer_gate = gaussian(key_list[0], (TOKENS, D), 1.0, 6.0, ((0, 8), (1, 4)))
    inner_gate = gaussian(key_list[1], (TOKENS, D), 1.0, 6.0, ((0, 8), (1, 4)))
    conv_value = gaussian(key_list[2], (TOKENS, D), 1.0, 6.0, ((0, 8), (1, 4)))
    conv_taps = gaussian(key_list[3], (KERNEL, D), KERNEL ** -0.5, 3.5, ((1, 4),))
    mix_out = draw_mix_out(jax.random.fold_in(key_list[18], 71), 0)
    gain_mixer = jnp.clip(1.0 + 0.18 * jax.random.normal(key_list[5], (D,), jnp.float32), 0.099609375, 1.8984375).astype(jnp.bfloat16)
    bias_mixer = gaussian(key_list[6], (D,), 0.5, 3.0, ((0, 4),))
    moe_input = gaussian(key_list[7], (TOKENS, D), 1.0, 6.0, ((0, 8),))
    route_ids_keys = jax.random.split(jax.random.fold_in(key_list[8], 1), TOKENS // ROWS)
    route_ids_turns = jax.random.permutation(jax.random.fold_in(key_list[8], 3), TOKENS // ROWS)
    route_ids = jax.vmap(lambda own, number: assign_block(jax.random.fold_in(key_list[8], 2), own, number, ROWS, EXPERTS, TOPK, CAP, 1))(route_ids_keys, route_ids_turns).reshape((TOKENS, TOPK))
    route_weights = jnp.clip(0.1 + 1.1 * jax.random.uniform(key_list[9], (TOKENS, TOPK), jnp.float32) ** level_of(key_list[9], (TOKENS, TOPK), ((0, 8),), -0.2, 0.2), 0.1, 1.2)
    expert_gate = gaussian(key_list[10], (EXPERTS, D, EFF), D ** -0.5, 0.125, ((0, 8), (2, 4)))
    expert_up = gaussian(key_list[11], (EXPERTS, D, EFF), D ** -0.5, 0.125, ((0, 8), (2, 4)))
    expert_down = draw_expert_down(jax.random.fold_in(key_list[18], 71), 0)
    shared_gate = gaussian(key_list[13], (D, SFF), D ** -0.5, 0.125, ((1, 4),))
    shared_up = gaussian(key_list[14], (D, SFF), D ** -0.5, 0.125, ((1, 4),))
    shared_down = draw_shared_down(jax.random.fold_in(key_list[18], 71), 0)
    gain_experts = jnp.clip(1.0 + 0.18 * jax.random.normal(key_list[16], (D,), jnp.float32), 0.099609375, 1.8984375).astype(jnp.bfloat16)
    bias_experts = gaussian(key_list[17], (D,), 0.5, 3.0, ((0, 4),))
    return {"outer_gate": outer_gate, "inner_gate": inner_gate, "conv_value": conv_value, "conv_taps": conv_taps, "mix_out": mix_out, "gain_mixer": gain_mixer, "bias_mixer": bias_mixer, "moe_input": moe_input, "route_ids": route_ids, "route_weights": route_weights, "expert_gate": expert_gate, "expert_up": expert_up, "expert_down": expert_down, "shared_gate": shared_gate, "shared_up": shared_up, "shared_down": shared_down, "gain_experts": gain_experts, "bias_experts": bias_experts}


def row_norm(values, gain, offset_bias):
    average = lax.optimization_barrier(jnp.mean(values, axis=1, keepdims=True))
    spread = lax.optimization_barrier(jnp.mean(values * values, axis=1, keepdims=True)) - average * average
    scaled = (values - average) * lax.rsqrt(spread + 1e-05)
    return (scaled * gain.astype(jnp.float32) + offset_bias.astype(jnp.float32)).astype(jnp.bfloat16)

def rounded(value):
    narrow = lax.optimization_barrier(value.astype(jnp.bfloat16))
    return narrow.astype(jnp.float32)

def reference(outer_gate, inner_gate, conv_value, conv_taps, mix_out, gain_mixer, bias_mixer, moe_input, route_ids, route_weights, expert_gate, expert_up, expert_down, shared_gate, shared_up, shared_down, gain_experts, bias_experts):
    product = rounded(inner_gate.astype(jnp.float32) * conv_value.astype(jnp.float32))
    length = product.shape[0]
    places = jnp.arange(length, dtype=jnp.int32) % SEQ_LEN
    convolved = jnp.zeros(product.shape, jnp.float32)
    for offset in range(KERNEL):
        delay_rows = KERNEL - 1 - offset
        delayed = jnp.pad(product, ((delay_rows, 0), (0, 0)))[:length]
        kept_mask = (places >= delay_rows).astype(jnp.float32)[:, None]
        convolved = convolved + conv_taps[offset].astype(jnp.float32)[None, :] * delayed * kept_mask
    weighted_in = (outer_gate.astype(jnp.float32) * convolved).astype(jnp.bfloat16)
    mixed = jnp.dot(weighted_in, mix_out, preferred_element_type=jnp.float32)
    out_mixer = row_norm(mixed, gain_mixer, bias_mixer)
    flat_ids = route_ids.reshape(-1).astype(jnp.int32)
    count_all = flat_ids.shape[0]
    order = jnp.argsort(flat_ids, stable=True).astype(jnp.int32)
    marks = (flat_ids[:, None] == jnp.arange(EXPERTS, dtype=jnp.int32)[None, :]).astype(jnp.int32)
    counts = lax.optimization_barrier(jnp.sum(marks, axis=0)).astype(jnp.int32)
    starts = (jnp.cumsum(counts) - counts).astype(jnp.int32)
    most_rows = N_EP * CAP

    def one_expert(results, expert):
        slots = jnp.arange(most_rows, dtype=jnp.int32)
        picks = jnp.clip(starts[expert] + slots, 0, count_all - 1).astype(jnp.int32)
        assigned = order[picks]
        valid = slots < counts[expert]
        inputs = moe_input[assigned // TOPK]
        gate_value = jnp.dot(inputs, expert_gate[expert], preferred_element_type=jnp.float32)
        up_value = jnp.dot(inputs, expert_up[expert], preferred_element_type=jnp.float32)
        hidden = (jax.nn.silu(gate_value) * up_value).astype(jnp.bfloat16)
        output = jnp.dot(hidden, expert_down[expert], preferred_element_type=jnp.float32).astype(jnp.bfloat16)
        target = jnp.where(valid, assigned, count_all).astype(jnp.int32)
        return (results.at[target].set(output, mode='drop'), None)
    empty = jnp.zeros((count_all, D), jnp.bfloat16)
    routed = lax.scan(one_expert, empty, jnp.arange(EXPERTS, dtype=jnp.int32))[0]
    shared_gate_value = jnp.dot(moe_input, shared_gate, preferred_element_type=jnp.float32)
    shared_up_value = jnp.dot(moe_input, shared_up, preferred_element_type=jnp.float32)
    shared_hidden = (jax.nn.silu(shared_gate_value) * shared_up_value).astype(jnp.bfloat16)
    shared_sum = jnp.dot(shared_hidden, shared_down, preferred_element_type=jnp.float32)
    weighted = routed.reshape(-1, TOPK, D).astype(jnp.float32) * route_weights.astype(jnp.float32)[:, :, None]
    combined = lax.optimization_barrier(jnp.sum(weighted, axis=1)) + shared_sum
    out_experts = row_norm(combined, gain_experts, bias_experts)
    return (out_mixer, out_experts)
```

```python
import functools
import types

import jax
import jax.numpy as jnp
from jax import lax
from jax.experimental import pallas as pl
from jax.experimental.pallas import tpu as pltpu
from jax.sharding import PartitionSpec as P

SEQS = 1


def shifted(block, axis, distance):
    devices = range(lax.axis_size(axis))
    route = [(i - distance, i) for i in devices if i - distance in devices]
    return lax.ppermute(block, axis, route)


def finish(values, totals, squares, full_width, gain, offset_bias):
    average = (totals / full_width)[:, None]
    spread = (squares / full_width)[:, None] - average * average
    scaled = (values - average) * lax.rsqrt(spread + 1e-05)
    return (scaled * gain.astype(jnp.float32) + offset_bias.astype(jnp.float32)).astype(
        jnp.bfloat16
    )


def plain_device(
    outer_gate,
    inner_gate,
    conv_value,
    conv_taps,
    mix_out,
    gain_mixer,
    bias_mixer,
    moe_input,
    route_ids,
    route_weights,
    expert_gate,
    expert_up,
    expert_down,
    shared_gate,
    shared_up,
    shared_down,
    gain_experts,
    bias_experts,
):
    token_rows = outer_gate.shape[0]
    column_count = outer_gate.shape[1]
    ep_count = lax.axis_size("ep")
    tp_count = lax.axis_size("tp")
    taps_count = conv_taps.shape[0]
    product = (inner_gate.astype(jnp.float32) * conv_value.astype(jnp.float32)).astype(jnp.bfloat16)
    border = shifted(product[token_rows - (taps_count - 1) :], "ep", 1)
    extended = jnp.concatenate([border, product], axis=0).astype(jnp.float32)
    seq_length = token_rows * ep_count // SEQS
    places = (
        lax.axis_index("ep") * token_rows + jnp.arange(token_rows, dtype=jnp.int32)
    ) % seq_length
    convolved = jnp.zeros((token_rows, column_count), jnp.float32)
    for offset in range(taps_count):
        delay_rows = taps_count - 1 - offset
        delayed = extended[offset : offset + token_rows]
        kept_mask = (places >= delay_rows).astype(jnp.float32)[:, None]
        convolved = convolved + conv_taps[offset].astype(jnp.float32)[None, :] * delayed * kept_mask
    weighted_in = (outer_gate.astype(jnp.float32) * convolved).astype(jnp.bfloat16)
    block = mix_out
    mixed = jnp.dot(
        lax.all_gather(weighted_in, "tp", axis=1, tiled=True),
        block,
        preferred_element_type=jnp.float32,
    )
    topk_count = route_ids.shape[1]
    local_experts = expert_gate.shape[0]
    expert_count = local_experts * ep_count
    capacity = max(2, 3 * token_rows * topk_count // (2 * expert_count))
    flat_ids = route_ids.reshape(-1)
    marks = (flat_ids[:, None] == jnp.arange(expert_count, dtype=jnp.int32)[None, :]).astype(
        jnp.int32
    )
    ranks = jnp.sum((jnp.cumsum(marks, axis=0) - marks) * marks, axis=1)
    targets = flat_ids * capacity + ranks
    sources = jnp.arange(flat_ids.shape[0], dtype=jnp.int32) // topk_count
    sent_rows = lax.dynamic_slice_in_dim(
        moe_input, lax.axis_index("tp") * column_count, column_count, 1
    )
    buffer_rows = jnp.zeros((expert_count * capacity, sent_rows.shape[1]), jnp.bfloat16)
    buffer_rows = buffer_rows.at[targets].set(sent_rows[sources])
    sectioned = buffer_rows.reshape(ep_count, local_experts * capacity, sent_rows.shape[1])
    arrived = lax.all_to_all(sectioned, "ep", split_axis=0, concat_axis=0, tiled=True)
    arrived = lax.all_gather(arrived, "tp", axis=2, tiled=True)
    expert_rows = arrived.reshape(ep_count, local_experts, capacity, arrived.shape[2])
    gate_value = jnp.einsum(
        "secd,edf->secf", expert_rows, expert_gate, preferred_element_type=jnp.float32
    )
    up_value = jnp.einsum(
        "secd,edf->secf", expert_rows, expert_up, preferred_element_type=jnp.float32
    )
    hidden = (jax.nn.silu(gate_value) * up_value).astype(jnp.bfloat16)
    flat_hidden = hidden.reshape(expert_count * capacity, hidden.shape[3])
    shared_gate_value = jnp.dot(moe_input, shared_gate, preferred_element_type=jnp.float32)
    shared_up_value = jnp.dot(moe_input, shared_up, preferred_element_type=jnp.float32)
    shared_hidden = (jax.nn.silu(shared_gate_value) * shared_up_value).astype(jnp.bfloat16)
    piece = lax.all_gather(flat_hidden, "tp", axis=1, tiled=True)
    block = expert_down
    shaped = piece.reshape(ep_count, local_experts, capacity, piece.shape[1])
    routed_sum = jnp.einsum("secf,efd->secd", shaped, block, preferred_element_type=jnp.float32)
    block = shared_down
    shared_sum = jnp.dot(
        lax.all_gather(shared_hidden, "tp", axis=1, tiled=True),
        block,
        preferred_element_type=jnp.float32,
    )
    expert_out = routed_sum.astype(jnp.bfloat16).reshape(
        ep_count, local_experts * capacity, column_count
    )
    returned = lax.all_to_all(expert_out, "ep", split_axis=0, concat_axis=0, tiled=True)
    picked = returned.reshape(expert_count * capacity, column_count)[targets].astype(jnp.float32)
    weighted = picked.reshape(token_rows, topk_count, column_count) * route_weights[:, :, None]
    combined = jnp.sum(weighted, axis=1) + shared_sum
    mixer_total, mixer_square, expert_total, expert_square = lax.psum(
        (
            jnp.sum(mixed, axis=1),
            jnp.sum(mixed * mixed, axis=1),
            jnp.sum(combined, axis=1),
            jnp.sum(combined * combined, axis=1),
        ),
        "tp",
    )
    full_width = column_count * tp_count
    out_mixer = finish(mixed, mixer_total, mixer_square, full_width, gain_mixer, bias_mixer)
    out_experts = finish(
        combined, expert_total, expert_square, full_width, gain_experts, bias_experts
    )
    return (out_mixer, out_experts)


PLANE = 2
CORES = 2
VMEM_BYTES = 60 * 1024 * 1024


(
    UP,
    DOWN,
    NEAR,
    ROUTE,
    PAIR,
    EDGE,
    CROSS,
    HIDDEN,
    SHARED,
    MIXER,
    PART,
    RETURN,
    STATS,
    ONWARD,
) = range(14)
LINE = 4
WHOLE = (3,)
ALL, INNER, OUTER = range(3)


def plan(act):
    return [
        (ALL, act.shared, ()),
        (ALL, act.up, (0,)),
        (ALL, act.start_y, (0,)),
        (ALL, act.line, (1, 0)),
        (INNER, act.line, (2, 0)),
        (ALL, act.start_x, (0,)),
        (ALL, act.line, (1, 1)),
        (INNER, act.line, (2, 1)),
        (OUTER, act.line, (2, 0)),
        (INNER, act.line, (3, 0)),
        (ALL, act.cross, (1, 2)),
        (ALL, act.cross, (1, 3)),
        (OUTER, act.line, (2, 1)),
        (INNER, act.line, (3, 1)),
        (INNER, act.cross, (2, 2)),
        (ALL, act.shared_relay, ()),
        (ALL, act.up, (1,)),
        (ALL, act.start, (1,)),
        (INNER, act.cross, (2, 3)),
        (OUTER, act.line, (3, 0)),
        (OUTER, act.cross, (2, 2)),
        (INNER, act.cross, (3, 2)),
        (OUTER, act.cross, (2, 3)),
        (OUTER, act.line, (3, 1)),
        (ALL, act.up, (2,)),
        (ALL, act.start, (2,)),
        (INNER, act.cross, (3, 3)),
        (ALL, act.relay, (1,)),
        (ALL, act.shared_dot, ()),
        (OUTER, act.cross, (3, 2)),
        (OUTER, act.cross, (3, 3)),
        (ALL, act.up_part, (3, 0)),
        (ALL, act.start_part, (3, 0)),
        (ALL, act.relay, (2,)),
        (ALL, act.up_part, (3, 1)),
        (ALL, act.start_part, (3, 1)),
        (ALL, act.down, (1,)),
        (ALL, act.give_back, (1,)),
        (ALL, act.relay_part, (3, 0)),
        (ALL, act.down, (2,)),
        (ALL, act.relay_part, (3, 1)),
        (ALL, act.give_back, (2,)),
        (ALL, act.mixer, ()),
        (ALL, act.relay, (0,)),
        (ALL, act.down_part, (3, 0)),
        (ALL, act.give_back_part, (3, 0)),
        (ALL, act.down_part, (3, 1)),
        (ALL, act.give_back_part, (3, 1)),
        (ALL, act.mixer_relay, ()),
        (ALL, act.down, (0,)),
        (ALL, act.give_back, (0,)),
        (ALL, act.mixer_dot, ()),
        (ALL, act.collect, (1,)),
        (ALL, act.collect, (2,)),
        (ALL, act.collect, (3,)),
    ]


def nearest_first(chips):
    def key(z):
        return lambda k: (abs(k - z), abs(2 * k - (chips - 1)))

    return [sorted((k for k in range(chips) if k != z), key=key(z)) for z in range(chips)]


def silu(value):
    return value / (1.0 + jnp.exp(-value))


def fused_kernel(
    shape,
    outer_hbm,
    inner_hbm,
    value_hbm,
    taps_hbm,
    mix_hbm,
    gain_m_hbm,
    bias_m_hbm,
    moe_hbm,
    ids_hbm,
    route_w_hbm,
    gate_hbm,
    up_hbm,
    down_hbm,
    shared_gate_hbm,
    shared_up_hbm,
    shared_down_hbm,
    gain_e_hbm,
    bias_e_hbm,
    out_m_hbm,
    out_e_hbm,
    out_m_ref,
    out_e_ref,
    outer_ref,
    inner_ref,
    value_ref,
    taps_ref,
    ids_ref,
    route_w_ref,
    gain_m_ref,
    bias_m_ref,
    gain_e_ref,
    bias_e_ref,
    mix_v,
    gate_v,
    up_v,
    down_v,
    shared_gate_v,
    shared_up_v,
    shared_down_v,
    tokens,
    route,
    rows_in,
    hidden,
    weighted,
    shared_hidden,
    border,
    edge,
    extended,
    peer_part,
    own_part,
    sent_sum,
    returned,
    stats_out,
    stats_in,
    mixed_ref,
    total_ref,
    load_sem,
    out_sem,
    send_sem,
    recv_sem,
    line_recv,
    route_recv,
    return_recv,
):
    ep_count, tp_count, capacity, seq_length = shape
    chips = ep_count // CORES
    rows, cols = outer_ref.shape
    full_width = cols * tp_count
    me = lax.axis_index("ep")
    j = lax.axis_index("tp")
    z = me // CORES
    c = me % CORES
    x = j % PLANE
    y = j // PLANE
    jx = y * PLANE + (1 - x)
    jy = (1 - y) * PLANE + x
    jd = (1 - y) * PLANE + (1 - x)
    other = z * CORES + (1 - c)
    f32, bf16 = jnp.float32, jnp.bfloat16

    orders = nearest_first(chips)

    def pick(values):
        chosen = jnp.int32(values[0])
        for k in range(1, chips):
            chosen = jnp.where(z == k, values[k], chosen)
        return chosen

    sources = [z] + [pick([orders[k][s - 1] for k in range(chips)]) for s in range(1, chips)]

    def onward_of(k, s):
        q = orders[k][s - 1]
        n = k + 1 if q < k else k - 1
        there = 0 <= n < chips
        return n if there else k, there, there and orders[n].index(q) + 1 in WHOLE

    stores = (
        pltpu.make_async_copy(out_m_ref, out_m_hbm, out_sem.at[0]),
        pltpu.make_async_copy(out_e_ref, out_e_hbm, out_sem.at[1]),
    )
    loads = []

    def load(source, target):
        loads.append(pltpu.make_async_copy(source, target, load_sem.at[len(loads)]))
        loads[-1].start()
        return loads[-1]

    barrier = pltpu.get_barrier_semaphore()
    for step in range(1, ep_count):
        pl.semaphore_signal(barrier, inc=1, device_id=((me + step) % ep_count, j), device_id_type=pl.DeviceIdType.MESH)
    for peer in (jx, jy, jd):
        pl.semaphore_signal(barrier, inc=1, device_id=(me, peer), device_id_type=pl.DeviceIdType.MESH)

    moe_load = load(moe_hbm, tokens.at[z, 0])
    ids_load = load(ids_hbm, ids_ref)
    route_w_load = load(route_w_hbm, route_w_ref)
    inner_load = load(inner_hbm, inner_ref)
    value_load = load(value_hbm, value_ref)
    shared_gate_load = load(shared_gate_hbm, shared_gate_v)
    shared_up_load = load(shared_up_hbm, shared_up_v)
    gate_load = load(gate_hbm.at[0], gate_v)
    up_load = load(up_hbm.at[0], up_v)
    outer_load = load(outer_hbm, outer_ref)
    taps_load = load(taps_hbm, taps_ref)
    gain_m_load = load(gain_m_hbm, gain_m_ref)
    bias_m_load = load(bias_m_hbm, bias_m_ref)
    gain_e_load = load(gain_e_hbm, gain_e_ref)
    bias_e_load = load(bias_e_hbm, bias_e_ref)
    shared_down_load = load(shared_down_hbm, shared_down_v)
    down_load = load(down_hbm.at[0], down_v)
    mix_load = load(mix_hbm, mix_v)

    def loaded(*several):
        for one in several:
            one.wait()

    loaded(ids_load, route_w_load)
    named = lax.broadcasted_iota(jnp.int32, (ep_count, rows), 0)
    dense = jnp.zeros((ep_count, rows), f32)
    for k in range(ids_ref.shape[0]):
        dense = dense + jnp.where(named == ids_ref[k : k + 1, :], route_w_ref[k : k + 1, :], 0.0)
    route[z, 0] = dense
    loaded(inner_load, value_load)
    product = (inner_ref[...].astype(f32) * value_ref[...].astype(f32)).astype(bf16)
    edge_rows = edge.shape[0]
    edge[...] = product[rows - edge_rows :]
    pad = extended.shape[0] - rows
    extended[pad:, :] = product.astype(f32)
    loaded(moe_load)

    with jax.named_scope("barrier"):
        pl.semaphore_wait(barrier, ep_count - 1 + tp_count - 1)

    groups = {}
    numbers = {}

    def remote(source, target, sent, received, device):
        return pltpu.make_async_remote_copy(
            src_ref=source,
            dst_ref=target,
            send_sem=sent,
            recv_sem=received,
            device_id=device,
            device_id_type=pl.DeviceIdType.MESH,
        )

    def group(name):
        return send_sem.at[groups.setdefault(name, len(groups))]

    def number(name):
        return recv_sem.at[numbers.setdefault(name, len(numbers))]

    def send(many, name, source, target, device, received=None, when=None):
        copy = remote(source, target, group(many), number(name) if received is None else received, device)
        if when is None:
            copy.start()
        else:
            pl.when(when)(copy.start)

    def arrive(name, target, received=None):
        remote(target, target, group(EDGE), number(name) if received is None else received, (other, j)).wait_recv()

    def sent(many, ref, when=None):
        def wait():
            remote(ref, ref, group(many), number(EDGE), (other, j)).wait_send()

        if when is None:
            wait()
        else:
            pl.when(when)(wait)

    def columns(owner):
        return pl.ds(pl.multiple_of(owner * cols, cols), cols)

    def gather_x(name, ref):
        part = ref.at[:, columns(j)]
        send(name[0], name + (0,), part, part, (me, jx))

    def gather_y(name, ref):
        part = ref.at[:, columns(j)]
        send(name[0], name + (1,), part, part, (me, jy))

    def relay_x(name, ref):
        half = ref.shape[0] // 2
        arrive(name + (0,), ref.at[:, columns(jx)])
        part = ref.at[pl.ds(0, half), columns(jx)]
        send(name[0], name + (2,), part, part, (me, jy))

    def relay_y(name, ref):
        half = ref.shape[0] // 2
        arrive(name + (1,), ref.at[:, columns(jy)])
        part = ref.at[pl.ds(half, half), columns(jy)]
        send(name[0], name + (2,), part, part, (me, jx))

    def gather_finish(name, ref):
        arrive(name + (2,), ref.at[:, columns(jd)])

    above = (z + 1) % chips
    below = (z + chips - 1) % chips
    quarters = (x, PLANE + y, 1 - x, PLANE + 1 - y)
    for k, quarter in enumerate(quarters[:PLANE]):
        part = tokens.at[z, 0, :, columns(quarter)]
        received = line_recv.at[z, k]
        send(UP, (), part, part, (above * CORES + c, j), received, z + 1 < chips)
        send(DOWN, (), part, part, (below * CORES + c, j), received, z > 0)
    send(NEAR, (), route.at[z, 0], route.at[z, 1], (other, j), route_recv.at[z])
    send(PAIR, (PAIR, 0), tokens.at[z, 0], tokens.at[z, 1], (other, j))
    for s in range(1, chips):
        target = (z + s) % chips
        for p in range(CORES):
            device = (target * CORES + (c if p == 0 else 1 - c), j)
            send(ROUTE, (), route.at[z, 0], route.at[z, p], device, route_recv.at[z])
    send(EDGE, EDGE, edge, border, ((me + 1) % ep_count, j))

    def dot(a, b):
        return jnp.dot(a, b, preferred_element_type=f32)

    def choice(s, p):
        weight = route[sources[s], p, pl.ds(me, 1), :]
        routed = (weight > 0.0).astype(f32)
        earlier = lax.broadcasted_iota(jnp.int32, (rows, rows), 0)
        later = lax.broadcasted_iota(jnp.int32, (rows, rows), 1)
        upper = (earlier <= later).astype(f32).astype(bf16)
        many = jnp.broadcast_to(routed, (16, rows)).astype(bf16)
        rank = dot(many, upper)[0:1, :] * routed
        slot = lax.broadcasted_iota(jnp.int32, (capacity, rows), 0).astype(f32) + 1.0
        return (slot == rank).astype(f32), weight

    def line_arrival(s, k):
        q = sources[s]
        quarter = quarters[k]
        part = tokens.at[q, 0, :, columns(quarter)]
        arrive((), part, line_recv.at[q, k])
        onward_send(s, k)
        if s not in WHOLE:
            send(CROSS, (CROSS, s, k), part, part, (me, (jx, jy)[k]))
        send(PAIR, (PAIR, s), part, tokens.at[q, 1, :, columns(quarter)], (other, j))

    onwards = {}
    for s in range(1, chips):
        for k in range(tp_count):
            told = [onward_of(n, s)[1 if k < PLANE else 2] for n in range(chips)]
            if any(told):
                onward = pick([onward_of(n, s)[0] for n in range(chips)])
                onwards[s, k] = (onward, pick([int(t) for t in told]) > 0)

    def onward_send(s, k):
        q = sources[s]
        part = tokens.at[q, 0, :, columns(quarters[k])]
        if (s, k) in onwards:
            onward, more = onwards[s, k]
            device = (onward * CORES + c, j)
            send((ONWARD, s, k - k % PLANE), (), part, part, device, line_recv.at[q, k], more)

    def cross_arrival(s, k):
        if s in WHOLE:
            line_arrival(s, k)
            return
        q = sources[s]
        part = tokens.at[q, 0, :, columns(quarters[k])]
        arrive((CROSS, s, k - PLANE), part)
        onward_send(s, k)
        send(PAIR, (PAIR, s), part, tokens.at[q, 1, :, columns(quarters[k])], (other, j))

    def expert_up(s):
        q = sources[s]
        arrive((), route.at[q] if s else route.at[q, 1], route_recv.at[q])
        if s == 0:
            loaded(gate_load, up_load)
        for p in range(CORES):
            picks, _ = choice(s, p)
            if p == 1:
                arrive((PAIR, s), tokens.at[q, 1])
            rows_in[p * capacity : (p + 1) * capacity, :] = dot(
                picks.astype(bf16), tokens[q, p]
            ).astype(bf16)
        held = silu(dot(rows_in[...], gate_v[...])) * dot(rows_in[...], up_v[...])
        hidden[q, :, columns(j)] = held.astype(bf16)

    def up_part(s, t):
        q = sources[s]
        p = (t + c) % CORES
        if t == 0:
            arrive((), route.at[q], route_recv.at[q])
            arrive((PAIR, s), tokens.at[q, 1])
        picks, _ = choice(s, p)
        taken = dot(picks.astype(bf16), tokens[q, p]).astype(bf16)
        held = silu(dot(taken, gate_v[...])) * dot(taken, up_v[...])
        hidden[q, t * capacity : (t + 1) * capacity, columns(j)] = held.astype(bf16)

    def part_ref(s, t):
        return hidden.at[sources[s], pl.ds(t * capacity, capacity)]

    def down_part(s, t):
        q = sources[s]
        gather_finish((HIDDEN, s, t), part_ref(s, t))
        picks, weight = choice(s, (t + c) % CORES)
        full = dot(hidden[q, t * capacity : (t + 1) * capacity], down_v[...])
        scale = jnp.sum(picks * weight, axis=1, keepdims=True)
        scaled = (full * scale).astype(bf16)
        spread = lax.dot_general(
            picks.astype(bf16), scaled, (((0,), (0,)), ((), ())), preferred_element_type=f32
        ).astype(bf16)

        @pl.when(c == t)
        def _():
            sent_sum[q] = spread

        @pl.when(c != t)
        def _():
            own_part[q] = spread
            send(PART, (PART, s), own_part.at[q], peer_part.at[q], (other, j))

    def return_part(s, t):
        @pl.when(c == t)
        def _():
            expert_return(s)

    def start_x(s):
        gather_x((HIDDEN, s), hidden.at[sources[s]])

    def start_y(s):
        gather_y((HIDDEN, s), hidden.at[sources[s]])

    def start(s):
        start_x(s)
        start_y(s)

    def relay(s):
        relay_x((HIDDEN, s), hidden.at[sources[s]])
        relay_y((HIDDEN, s), hidden.at[sources[s]])

    def start_part(s, t):
        gather_x((HIDDEN, s, t), part_ref(s, t))
        gather_y((HIDDEN, s, t), part_ref(s, t))

    def relay_part(s, t):
        relay_x((HIDDEN, s, t), part_ref(s, t))
        relay_y((HIDDEN, s, t), part_ref(s, t))

    def collect(s):
        q = sources[s]
        arrive((), returned.at[q], return_recv.at[q])
        total_ref[...] = total_ref[...] + returned[q].astype(f32)

    def expert_down(s):
        q = sources[s]
        gather_finish((HIDDEN, s), hidden.at[q])
        full = dot(hidden[q], down_v[...])
        for p in reversed(range(CORES)):
            picks, weight = choice(s, p)
            scale = jnp.sum(picks * weight, axis=1, keepdims=True)
            scaled = (full[p * capacity : (p + 1) * capacity] * scale).astype(bf16)
            spread = lax.dot_general(
                picks.astype(bf16), scaled, (((0,), (0,)), ((), ())), preferred_element_type=f32
            )
            if p == 1:
                own_part[q] = spread.astype(bf16)
                send(PART, (PART, s), own_part.at[q], peer_part.at[q], (other, j))
            elif s == 0:
                total_ref[...] = total_ref[...] + spread
            else:
                sent_sum[q] = spread.astype(bf16)

    def expert_return(s):
        q = sources[s]
        arrive((PART, s), peer_part.at[q])
        if s == 0:
            total_ref[...] = total_ref[...] + peer_part[q].astype(f32)
        else:
            sent_sum[q] = (sent_sum[q].astype(f32) + peer_part[q].astype(f32)).astype(bf16)
            send(RETURN, (), sent_sum.at[q], returned.at[z], (q * CORES + c, j), return_recv.at[z])

    def stats_start(k, values):
        lane = lax.broadcasted_iota(jnp.int32, (rows, rows), 1)
        total = jnp.sum(values, axis=1, keepdims=True)
        square = jnp.sum(values * values, axis=1, keepdims=True)
        tile = jnp.where(lane == 0, total, jnp.where(lane == 1, square, 0.0))
        stats_out[k] = tile.T[0 : stats_out.shape[1], :]
        for n, peer in enumerate((jx, jy, jd)):
            send((STATS, k), (STATS, k), stats_out.at[k], stats_in.at[k, n], (me, peer))

    def stats_finish(k, values, gain_ref, bias_ref, out_ref):
        tile = stats_out[k]
        arrive((STATS, k), stats_in.at[k])
        for n in range(tp_count - 1):
            tile = tile + stats_in[k, n]
        padded = jnp.concatenate(
            [tile, jnp.zeros((rows - tile.shape[0], rows), f32)], axis=0
        ).T
        average = padded[:, 0:1] / full_width
        spread = padded[:, 1:2] / full_width - average * average
        scaled = (values - average) * lax.rsqrt(spread + 1e-05)
        out_ref[...] = (
            scaled * gain_ref[...].astype(f32).reshape(1, cols)
            + bias_ref[...].astype(f32).reshape(1, cols)
        ).astype(bf16)

    def shared_start():
        loaded(shared_gate_load, shared_up_load)
        own = tokens[z, 0]
        held = silu(dot(own, shared_gate_v[...])) * dot(own, shared_up_v[...])
        shared_hidden[:, columns(j)] = held.astype(bf16)
        gather_x((SHARED,), shared_hidden)
        gather_y((SHARED,), shared_hidden)

    def mixer_start():
        arrive(EDGE, border)
        loaded(outer_load, taps_load)
        extended[pad - edge_rows : pad, :] = border[...].astype(f32)
        places = (me * rows + lax.broadcasted_iota(jnp.int32, (rows, 1), 0)) % seq_length
        taps_count = taps_ref.shape[0]
        convolved = jnp.zeros((rows, cols), f32)
        for offset in range(taps_count):
            delay = taps_count - 1 - offset
            delayed = extended[pad - delay : pad - delay + rows, :]
            kept = (places >= delay).astype(f32)
            convolved = convolved + taps_ref[offset : offset + 1, :].astype(f32) * delayed * kept
        weighted[:, columns(j)] = (outer_ref[...].astype(f32) * convolved).astype(bf16)
        gather_x((MIXER,), weighted)
        gather_y((MIXER,), weighted)

    def shared_relay():
        relay_x((SHARED,), shared_hidden)
        relay_y((SHARED,), shared_hidden)

    def mixer_relay():
        relay_x((MIXER,), weighted)
        relay_y((MIXER,), weighted)

    def mixer_dot():
        gather_finish((MIXER,), weighted)
        loaded(mix_load)
        mixed_ref[...] = dot(weighted[...], mix_v[...])
        stats_start(0, mixed_ref[...])

    def mixer_end():
        loaded(gain_m_load, bias_m_load, gain_e_load, bias_e_load)
        stats_finish(0, mixed_ref[...], gain_m_ref, bias_m_ref, out_m_ref)
        stores[0].start()

    def shared_dot():
        gather_finish((SHARED,), shared_hidden)
        loaded(shared_down_load, down_load)
        total_ref[...] = dot(shared_hidden[...], shared_down_v[...])

    act = types.SimpleNamespace(
        shared=shared_start,
        up=expert_up,
        start=start,
        start_x=start_x,
        start_y=start_y,
        line=line_arrival,
        cross=cross_arrival,
        relay=relay,
        down=expert_down,
        give_back=expert_return,
        up_part=up_part,
        start_part=start_part,
        relay_part=relay_part,
        down_part=down_part,
        give_back_part=return_part,
        shared_relay=shared_relay,
        shared_dot=shared_dot,
        mixer=mixer_start,
        mixer_relay=mixer_relay,
        mixer_dot=mixer_dot,
        collect=collect,
    )
    inner = (z > 0) & (z < chips - 1)
    for where, step, which in plan(act):
        if where == ALL:
            step(*which)
        else:
            pl.when(inner if where == INNER else ~inner)(functools.partial(step, *which))
    with jax.named_scope("stats"):
        stats_start(1, total_ref[...])
    with jax.named_scope("mixer_end"):
        mixer_end()
    with jax.named_scope("drain"):
        lines = tokens.at[0, 0, :, pl.ds(0, PLANE * cols)]
        sent(UP, lines, z + 1 < chips)
        sent(DOWN, lines, z > 0)
        for s, k in onwards:
            if k % PLANE == 0:
                sent((ONWARD, s, k), lines, onwards[s, k][1])
        sent(NEAR, route.at[0, 0])
        sent(PAIR, tokens.at[:, 0])
        sent(ROUTE, route.at[pl.ds(0, chips - 1)])
        sent(EDGE, edge)
        sent(CROSS, tokens.at[pl.ds(0, chips - 1 - len(WHOLE)), 0, :, pl.ds(0, PLANE * cols)])
        gathered = pl.ds(0, (tp_count - 1) * cols)
        sent(HIDDEN, hidden.at[:, :, gathered])
        sent(SHARED, shared_hidden.at[:, gathered])
        sent(MIXER, weighted.at[:, gathered])
        sent(PART, own_part)
        sent(RETURN, own_part.at[pl.ds(0, chips - 1)])
        sent((STATS, 0), stats_in.at[0])
    with jax.named_scope("finish"):
        stats_finish(1, total_ref[...], gain_e_ref, bias_e_ref, out_e_ref)
    stores[1].start()
    with jax.named_scope("sent"):
        sent((STATS, 1), stats_in.at[1])
        for store in stores:
            store.wait()


def pass_kernel(first_ref, second_ref, out_first_ref, out_second_ref):
    out_first_ref[...] = first_ref[...]
    out_second_ref[...] = second_ref[...]


def fused_device(
    outer_gate,
    inner_gate,
    conv_value,
    conv_taps,
    mix_out,
    gain_mixer,
    bias_mixer,
    moe_input,
    route_ids,
    route_weights,
    expert_gate,
    expert_up,
    expert_down,
    shared_gate,
    shared_up,
    shared_down,
    gain_experts,
    bias_experts,
):
    rows, cols = outer_gate.shape
    width = moe_input.shape[1]
    ep_count = lax.axis_size("ep")
    tp_count = lax.axis_size("tp")
    chips = ep_count // CORES
    capacity = max(2, 3 * rows * route_ids.shape[1] // (2 * ep_count))
    seq_length = rows * ep_count // SEQS
    bf16, f32 = jnp.bfloat16, jnp.float32
    vmem = pl.BlockSpec(memory_space=pltpu.VMEM)
    hbm = pl.BlockSpec(memory_space=pl.ANY)
    copies = 4 * chips + 20
    weight = pltpu.VMEM((width, cols), bf16)
    scratch = [
        *([pltpu.VMEM((rows, cols), bf16)] * 5),
        pltpu.VMEM(conv_taps.shape, bf16),
        pltpu.VMEM(route_ids.shape[::-1], jnp.int32),
        pltpu.VMEM(route_weights.shape[::-1], f32),
        *([pltpu.VMEM((cols,), bf16)] * 4),
        *([weight] * 7),
        pltpu.VMEM((chips, CORES, rows, width), bf16),
        pltpu.VMEM((chips, CORES, ep_count, rows), f32),
        pltpu.VMEM((CORES * capacity, width), bf16),
        pltpu.VMEM((chips, CORES * capacity, width), bf16),
        pltpu.VMEM((rows, width), bf16),
        pltpu.VMEM((rows, width), bf16),
        pltpu.VMEM((16, cols), bf16),
        pltpu.VMEM((16, cols), bf16),
        pltpu.VMEM((rows + 16, cols), f32),
        pltpu.VMEM((chips, rows, cols), bf16),
        pltpu.VMEM((chips, rows, cols), bf16),
        pltpu.VMEM((chips, rows, cols), bf16),
        pltpu.VMEM((chips, rows, cols), bf16),
        pltpu.VMEM((2, 8, rows), f32),
        pltpu.VMEM((2, tp_count - 1, 8, rows), f32),
        pltpu.VMEM((rows, cols), f32),
        pltpu.VMEM((rows, cols), f32),
        pltpu.SemaphoreType.DMA((18,)),
        pltpu.SemaphoreType.DMA((2,)),
        pltpu.SemaphoreType.DMA((chips + 15,)),
        pltpu.SemaphoreType.DMA((copies,)),
        pltpu.SemaphoreType.DMA((chips, tp_count)),
        pltpu.SemaphoreType.DMA((chips,)),
        pltpu.SemaphoreType.DMA((chips,)),
    ]
    out = jax.ShapeDtypeStruct((rows, cols), bf16)
    first, second = pl.pallas_call(
        functools.partial(fused_kernel, (ep_count, tp_count, capacity, seq_length)),
        out_shape=(out, out),
        in_specs=[hbm] * 18,
        out_specs=(hbm, hbm),
        scratch_shapes=scratch,
        compiler_params=pltpu.CompilerParams(
            collective_id=0, has_side_effects=True, vmem_limit_bytes=VMEM_BYTES
        ),
    )(
        outer_gate,
        inner_gate,
        conv_value,
        conv_taps,
        mix_out,
        gain_mixer,
        bias_mixer,
        moe_input,
        route_ids.T,
        route_weights.T,
        expert_gate,
        expert_up,
        expert_down,
        shared_gate,
        shared_up,
        shared_down,
        gain_experts,
        bias_experts,
    )
    return pl.pallas_call(
        pass_kernel, out_shape=(out, out), in_specs=[vmem, vmem], out_specs=(vmem, vmem)
    )(first, second)


def on_device(*arrays):
    local_experts = arrays[10].shape[0]
    square = lax.axis_size("tp") == PLANE * PLANE
    if square and local_experts == 1 and lax.axis_size("ep") == CORES * LINE:
        return fused_device(*arrays)
    return plain_device(*arrays)


def solution(mesh):
    in_specs = (
        P("ep", "tp"),
        P("ep", "tp"),
        P("ep", "tp"),
        P(None, "tp"),
        P(None, "tp"),
        P("tp"),
        P("tp"),
        P("ep", None),
        P("ep", None),
        P("ep", None),
        P("ep", None, "tp"),
        P("ep", None, "tp"),
        P("ep", None, "tp"),
        P(None, "tp"),
        P(None, "tp"),
        P(None, "tp"),
        P("tp"),
        P("tp"),
    )
    out_specs = (P("ep", "tp"), P("ep", "tp"))
    return jax.shard_map(
        on_device, mesh=mesh, in_specs=in_specs, out_specs=out_specs, check_vma=False
    )
```

```python
import functools
import types

import jax
import jax.numpy as jnp
from jax import lax
from jax.experimental import pallas as pl
from jax.experimental.pallas import tpu as pltpu
from jax.sharding import PartitionSpec as P

SEQS = 1


def shifted(block, axis, distance):
    devices = range(lax.axis_size(axis))
    route = [(i - distance, i) for i in devices if i - distance in devices]
    return lax.ppermute(block, axis, route)


def finish(values, totals, squares, full_width, gain, offset_bias):
    average = (totals / full_width)[:, None]
    spread = (squares / full_width)[:, None] - average * average
    scaled = (values - average) * lax.rsqrt(spread + 1e-05)
    return (scaled * gain.astype(jnp.float32) + offset_bias.astype(jnp.float32)).astype(
        jnp.bfloat16
    )


def plain_device(
    outer_gate,
    inner_gate,
    conv_value,
    conv_taps,
    mix_out,
    gain_mixer,
    bias_mixer,
    moe_input,
    route_ids,
    route_weights,
    expert_gate,
    expert_up,
    expert_down,
    shared_gate,
    shared_up,
    shared_down,
    gain_experts,
    bias_experts,
):
    token_rows = outer_gate.shape[0]
    column_count = outer_gate.shape[1]
    ep_count = lax.axis_size("ep")
    tp_count = lax.axis_size("tp")
    taps_count = conv_taps.shape[0]
    product = (inner_gate.astype(jnp.float32) * conv_value.astype(jnp.float32)).astype(jnp.bfloat16)
    border = shifted(product[token_rows - (taps_count - 1) :], "ep", 1)
    extended = jnp.concatenate([border, product], axis=0).astype(jnp.float32)
    seq_length = token_rows * ep_count // SEQS
    places = (
        lax.axis_index("ep") * token_rows + jnp.arange(token_rows, dtype=jnp.int32)
    ) % seq_length
    convolved = jnp.zeros((token_rows, column_count), jnp.float32)
    for offset in range(taps_count):
        delay_rows = taps_count - 1 - offset
        delayed = extended[offset : offset + token_rows]
        kept_mask = (places >= delay_rows).astype(jnp.float32)[:, None]
        convolved = convolved + conv_taps[offset].astype(jnp.float32)[None, :] * delayed * kept_mask
    weighted_in = (outer_gate.astype(jnp.float32) * convolved).astype(jnp.bfloat16)
    block = mix_out
    mixed = jnp.dot(
        lax.all_gather(weighted_in, "tp", axis=1, tiled=True),
        block,
        preferred_element_type=jnp.float32,
    )
    topk_count = route_ids.shape[1]
    local_experts = expert_gate.shape[0]
    expert_count = local_experts * ep_count
    capacity = max(2, 3 * token_rows * topk_count // (2 * expert_count))
    flat_ids = route_ids.reshape(-1)
    marks = (flat_ids[:, None] == jnp.arange(expert_count, dtype=jnp.int32)[None, :]).astype(
        jnp.int32
    )
    ranks = jnp.sum((jnp.cumsum(marks, axis=0) - marks) * marks, axis=1)
    targets = flat_ids * capacity + ranks
    sources = jnp.arange(flat_ids.shape[0], dtype=jnp.int32) // topk_count
    sent_rows = lax.dynamic_slice_in_dim(
        moe_input, lax.axis_index("tp") * column_count, column_count, 1
    )
    buffer_rows = jnp.zeros((expert_count * capacity, sent_rows.shape[1]), jnp.bfloat16)
    buffer_rows = buffer_rows.at[targets].set(sent_rows[sources])
    sectioned = buffer_rows.reshape(ep_count, local_experts * capacity, sent_rows.shape[1])
    arrived = lax.all_to_all(sectioned, "ep", split_axis=0, concat_axis=0, tiled=True)
    arrived = lax.all_gather(arrived, "tp", axis=2, tiled=True)
    expert_rows = arrived.reshape(ep_count, local_experts, capacity, arrived.shape[2])
    gate_value = jnp.einsum(
        "secd,edf->secf", expert_rows, expert_gate, preferred_element_type=jnp.float32
    )
    up_value = jnp.einsum(
        "secd,edf->secf", expert_rows, expert_up, preferred_element_type=jnp.float32
    )
    hidden = (jax.nn.silu(gate_value) * up_value).astype(jnp.bfloat16)
    flat_hidden = hidden.reshape(expert_count * capacity, hidden.shape[3])
    shared_gate_value = jnp.dot(moe_input, shared_gate, preferred_element_type=jnp.float32)
    shared_up_value = jnp.dot(moe_input, shared_up, preferred_element_type=jnp.float32)
    shared_hidden = (jax.nn.silu(shared_gate_value) * shared_up_value).astype(jnp.bfloat16)
    piece = lax.all_gather(flat_hidden, "tp", axis=1, tiled=True)
    block = expert_down
    shaped = piece.reshape(ep_count, local_experts, capacity, piece.shape[1])
    routed_sum = jnp.einsum("secf,efd->secd", shaped, block, preferred_element_type=jnp.float32)
    block = shared_down
    shared_sum = jnp.dot(
        lax.all_gather(shared_hidden, "tp", axis=1, tiled=True),
        block,
        preferred_element_type=jnp.float32,
    )
    expert_out = routed_sum.astype(jnp.bfloat16).reshape(
        ep_count, local_experts * capacity, column_count
    )
    returned = lax.all_to_all(expert_out, "ep", split_axis=0, concat_axis=0, tiled=True)
    picked = returned.reshape(expert_count * capacity, column_count)[targets].astype(jnp.float32)
    weighted = picked.reshape(token_rows, topk_count, column_count) * route_weights[:, :, None]
    combined = jnp.sum(weighted, axis=1) + shared_sum
    mixer_total, mixer_square, expert_total, expert_square = lax.psum(
        (
            jnp.sum(mixed, axis=1),
            jnp.sum(mixed * mixed, axis=1),
            jnp.sum(combined, axis=1),
            jnp.sum(combined * combined, axis=1),
        ),
        "tp",
    )
    full_width = column_count * tp_count
    out_mixer = finish(mixed, mixer_total, mixer_square, full_width, gain_mixer, bias_mixer)
    out_experts = finish(
        combined, expert_total, expert_square, full_width, gain_experts, bias_experts
    )
    return (out_mixer, out_experts)


PLANE = 2
SMALL_BYTES = 4 * 1024 * 1024
CORES = 2
VMEM_BYTES = 48 * 1024 * 1024


(
    UP,
    DOWN,
    ROUTE,
    PAIR,
    EDGE,
    CROSS,
    HIDDEN,
    SHARED,
    MIXER,
    PART,
    RETURN,
    STATS,
    ONWARD,
    ROUTE_UP,
    ROUTE_DOWN,
) = range(15)
LINE = 4
ALL, INNER, OUTER = range(3)


def plan(act):
    return [
        (ALL, act.shared, ()),
        (ALL, act.up, (0,)),
        (ALL, act.start_y, (0,)),
        (ALL, act.line, (1, 0, True)),
        (INNER, act.line, (2, 0)),
        (ALL, act.start_x, (0,)),
        (ALL, act.line, (1, 1, True)),
        (INNER, act.line, (2, 1)),
        (OUTER, act.line, (2, 0, True)),
        (INNER, act.line, (2, 2)),
        (INNER, act.line, (3, 0)),
        (ALL, act.cross, (1, 2)),
        (ALL, act.cross, (1, 3)),
        (INNER, act.line, (2, 3)),
        (OUTER, act.line, (2, 1, True)),
        (INNER, act.line, (3, 1)),
        (ALL, act.shared_relay, ()),
        (ALL, act.up, (1,)),
        (ALL, act.start, (1,)),
        (INNER, act.line, (3, 2)),
        (OUTER, act.line, (3, 0)),
        (OUTER, act.cross, (2, 2)),
        (OUTER, act.cross, (2, 3)),
        (OUTER, act.line, (3, 1)),
        (OUTER, act.relay, (0,)),
        (ALL, act.up, (2,)),
        (ALL, act.start, (2,)),
        (INNER, act.line, (3, 3)),
        (ALL, act.shared_dot, ()),
        (OUTER, act.line, (3, 2)),
        (OUTER, act.line, (3, 3)),
        (INNER, act.relay, (1,)),
        (INNER, act.relay, (2,)),
        (ALL, act.up_part, (3, 0)),
        (ALL, act.start_part, (3, 0)),
        (OUTER, act.relay, (2,)),
        (ALL, act.up_part, (3, 1)),
        (ALL, act.start_part, (3, 1)),
        (INNER, act.down, (1,)),
        (INNER, act.give_back, (1,)),
        (INNER, act.down, (2,)),
        (ALL, act.relay_part, (3, 0)),
        (INNER, act.give_back, (2,)),
        (OUTER, act.down, (2,)),
        (ALL, act.relay_part, (3, 1)),
        (OUTER, act.relay, (1,)),
        (OUTER, act.give_back, (2,)),
        (ALL, act.mixer, ()),
        (INNER, act.relay, (0,)),
        (ALL, act.down_part, (3, 0)),
        (ALL, act.give_back_part, (3, 0)),
        (ALL, act.down_part, (3, 1)),
        (ALL, act.give_back_part, (3, 1)),
        (OUTER, act.down, (1,)),
        (OUTER, act.give_back, (1,)),
        (ALL, act.mixer_relay, ()),
        (ALL, act.down, (0,)),
        (ALL, act.give_back, (0,)),
        (ALL, act.mixer_dot, ()),
        (ALL, act.collect, (1,)),
        (ALL, act.collect, (2,)),
        (ALL, act.collect, (3,)),
    ]


def nearest_first(chips):
    def key(z):
        return lambda k: (abs(k - z), abs(2 * k - (chips - 1)))

    return [sorted((k for k in range(chips) if k != z), key=key(z)) for z in range(chips)]


def silu(value):
    return value / (1.0 + jnp.exp(-value))


def fused_kernel(
    shape,
    outer_hbm,
    inner_hbm,
    value_hbm,
    taps_hbm,
    mix_hbm,
    gain_m_hbm,
    bias_m_hbm,
    moe_hbm,
    ids_hbm,
    route_w_hbm,
    gate_hbm,
    up_hbm,
    down_hbm,
    shared_gate_hbm,
    shared_up_hbm,
    shared_down_hbm,
    gain_e_hbm,
    bias_e_hbm,
    out_m_ref,
    out_e_ref,
    outer_ref,
    inner_ref,
    value_ref,
    taps_ref,
    ids_ref,
    route_w_ref,
    gain_m_ref,
    bias_m_ref,
    gain_e_ref,
    bias_e_ref,
    mix_v,
    gate_v,
    up_v,
    down_v,
    shared_gate_v,
    shared_up_v,
    shared_down_v,
    tokens,
    route,
    rows_in,
    hidden,
    weighted,
    shared_hidden,
    border,
    edge,
    extended,
    peer_part,
    own_part,
    sent_sum,
    returned,
    stats_out,
    stats_in,
    mixed_ref,
    total_ref,
    load_sem,
    send_sem,
    recv_sem,
    line_recv,
    route_recv,
    return_recv,
):
    ep_count, tp_count, capacity, seq_length = shape
    chips = ep_count // CORES
    rows, cols = outer_ref.shape
    full_width = cols * tp_count
    me = lax.axis_index("ep")
    j = lax.axis_index("tp")
    z = me // CORES
    c = me % CORES
    x = j % PLANE
    y = j // PLANE
    jx = y * PLANE + (1 - x)
    jy = (1 - y) * PLANE + x
    jd = (1 - y) * PLANE + (1 - x)
    other = z * CORES + (1 - c)
    f32, bf16 = jnp.float32, jnp.bfloat16

    orders = nearest_first(chips)

    def pick(values):
        chosen = jnp.int32(values[0])
        for k in range(1, chips):
            chosen = jnp.where(z == k, values[k], chosen)
        return chosen

    sources = [z] + [pick([orders[k][s - 1] for k in range(chips)]) for s in range(1, chips)]

    def whole(k, q):
        s = orders[k].index(q) + 1
        return s == chips - 1 or s == chips - 2 and 0 < k < chips - 1

    def onward_of(k, s):
        q = orders[k][s - 1]
        n = k + 1 if q < k else k - 1
        there = 0 <= n < chips
        return n if there else k, there, there and whole(n, q)

    rising = pick([int(k + 1 < chips and whole(k + 1, k)) for k in range(chips)]) > 0
    falling = pick([int(k > 0 and whole(k - 1, k)) for k in range(chips)]) > 0

    loads = []

    def load(source, target):
        loads.append(pltpu.make_async_copy(source, target, load_sem.at[len(loads)]))
        loads[-1].start()
        return loads[-1]

    above = (z + 1) % chips
    below = (z + chips - 1) % chips
    higher = z + 1 < chips
    lower = z > 0
    beside = jnp.where(c > 0, me + 1, me + ep_count - 1) % ep_count
    slanted = jnp.where(c > 0, z + 1 < chips, z > 0)

    barrier = pltpu.get_barrier_semaphore()

    def greet(row, column):
        pl.semaphore_signal(
            barrier, inc=1, device_id=(row, column), device_id_type=pl.DeviceIdType.MESH
        )

    greet(other, j)
    greet(me, jx)
    greet(me, jy)
    pl.when(higher)(lambda: greet(above * CORES + c, j))
    pl.when(lower)(lambda: greet(below * CORES + c, j))
    pl.when(slanted)(lambda: greet(beside, j))
    greeted = 3 + higher.astype(jnp.int32) + lower.astype(jnp.int32) + slanted.astype(jnp.int32)

    moe_load = load(moe_hbm, tokens.at[z, 0])
    ids_load = load(ids_hbm, ids_ref)
    route_w_load = load(route_w_hbm, route_w_ref)
    inner_load = load(inner_hbm, inner_ref)
    value_load = load(value_hbm, value_ref)
    shared_gate_load = load(shared_gate_hbm, shared_gate_v)
    shared_up_load = load(shared_up_hbm, shared_up_v)
    gate_load = load(gate_hbm.at[0], gate_v)
    up_load = load(up_hbm.at[0], up_v)
    outer_load = load(outer_hbm, outer_ref)
    taps_load = load(taps_hbm, taps_ref)
    gain_m_load = load(gain_m_hbm, gain_m_ref)
    bias_m_load = load(bias_m_hbm, bias_m_ref)
    gain_e_load = load(gain_e_hbm, gain_e_ref)
    bias_e_load = load(bias_e_hbm, bias_e_ref)
    shared_down_load = load(shared_down_hbm, shared_down_v)
    down_load = load(down_hbm.at[0], down_v)
    mix_load = load(mix_hbm, mix_v)

    def loaded(*several):
        for one in several:
            one.wait()

    loaded(moe_load)
    with jax.named_scope("barrier"):
        pl.semaphore_wait(barrier, greeted)

    groups = {}
    numbers = {}

    def remote(source, target, sent, received, device):
        return pltpu.make_async_remote_copy(
            src_ref=source,
            dst_ref=target,
            send_sem=sent,
            recv_sem=received,
            device_id=device,
            device_id_type=pl.DeviceIdType.MESH,
        )

    def group(name):
        return send_sem.at[groups.setdefault(name, len(groups))]

    def number(name):
        return recv_sem.at[numbers.setdefault(name, len(numbers))]

    def send(many, name, source, target, device, received=None, when=None):
        copy = remote(source, target, group(many), number(name) if received is None else received, device)
        if when is None:
            copy.start()
        else:
            pl.when(when)(copy.start)

    def arrive(name, target, received=None):
        remote(target, target, group(EDGE), number(name) if received is None else received, (other, j)).wait_recv()

    def sent(many, ref, when=None):
        def wait():
            remote(ref, ref, group(many), number(EDGE), (other, j)).wait_send()

        if when is None:
            wait()
        else:
            pl.when(when)(wait)

    def columns(owner):
        return pl.ds(pl.multiple_of(owner * cols, cols), cols)

    def gather_x(name, ref):
        part = ref.at[:, columns(j)]
        send(name[0], name + (0,), part, part, (me, jx))

    def gather_y(name, ref):
        part = ref.at[:, columns(j)]
        send(name[0], name + (1,), part, part, (me, jy))

    def relay_x(name, ref):
        half = ref.shape[0] // 2
        arrive(name + (0,), ref.at[:, columns(jx)])
        part = ref.at[pl.ds(0, half), columns(jx)]
        send(name[0], name + (2,), part, part, (me, jy))

    def relay_y(name, ref):
        half = ref.shape[0] // 2
        arrive(name + (1,), ref.at[:, columns(jy)])
        part = ref.at[pl.ds(half, half), columns(jy)]
        send(name[0], name + (2,), part, part, (me, jx))

    def gather_finish(name, ref):
        arrive(name + (2,), ref.at[:, columns(jd)])

    quarters = (x, PLANE + y, 1 - x, PLANE + 1 - y)
    def line_start(k):
        part = tokens.at[z, 0, :, columns(quarters[k])]
        received = line_recv.at[z, k]
        more = k - k % PLANE
        device = (above * CORES + c, j)
        send((UP, more), (), part, part, device, received, rising if more else higher)
        device = (below * CORES + c, j)
        send((DOWN, more), (), part, part, device, received, falling if more else lower)

    line_start(0)
    send(PAIR, (PAIR, 0), tokens.at[z, 0], tokens.at[z, 1], (other, j))
    loaded(ids_load, route_w_load)
    named = lax.broadcasted_iota(jnp.int32, (ep_count, rows), 0)
    dense = jnp.zeros((ep_count, rows), f32)
    for k in range(ids_ref.shape[0]):
        dense = dense + jnp.where(named == ids_ref[k : k + 1, :], route_w_ref[k : k + 1, :], 0.0)
    route[z, 0] = dense
    own = route.at[z, 0]
    send(ROUTE_UP, (), own, own, (above * CORES + c, j), route_recv.at[z], higher)
    send(ROUTE_DOWN, (), own, own, (below * CORES + c, j), route_recv.at[z], lower)
    send(ROUTE, (ROUTE, 0), own, route.at[z, 1], (other, j))
    line_start(1)
    line_start(2)
    line_start(3)
    loaded(inner_load, value_load)
    product = (inner_ref[...].astype(f32) * value_ref[...].astype(f32)).astype(bf16)
    edge_rows = edge.shape[0]
    edge[...] = product[rows - edge_rows :]

    @pl.when(me == 0)
    def _():
        border[...] = jnp.zeros_like(border)

    pad = extended.shape[0] - rows
    extended[pad:, :] = product.astype(f32)
    last = me == ep_count - 1
    send(EDGE, EDGE, edge, border, ((me + 1) % ep_count, j), None, ~last)

    def dot(a, b):
        return jnp.dot(a, b, preferred_element_type=f32)

    def choice(s, p):
        weight = route[sources[s], p, pl.ds(me, 1), :]
        routed = (weight > 0.0).astype(f32)
        earlier = lax.broadcasted_iota(jnp.int32, (rows, rows), 0)
        later = lax.broadcasted_iota(jnp.int32, (rows, rows), 1)
        upper = (earlier <= later).astype(f32).astype(bf16)
        many = jnp.broadcast_to(routed, (16, rows)).astype(bf16)
        rank = dot(many, upper)[0:1, :] * routed
        slot = lax.broadcasted_iota(jnp.int32, (capacity, rows), 0).astype(f32) + 1.0
        return (slot == rank).astype(f32), weight

    def line_arrival(s, k, swap=False):
        q = sources[s]
        quarter = quarters[k]
        part = tokens.at[q, 0, :, columns(quarter)]
        if k == 1:
            own = route.at[q, 0]
            arrive((), own, route_recv.at[q])
            if (s, k) in onwards:
                onward, more = onwards[s, k]
                device = (onward * CORES + c, j)
                send((ROUTE, s), (), own, own, device, route_recv.at[q], more)
            send(ROUTE, (ROUTE, s), own, route.at[q, 1], (other, j))
        arrive((), part, line_recv.at[q, k])
        onward_send(s, k)
        if swap:
            send((CROSS, s), (CROSS, s, k), part, part, (me, (jx, jy)[k]))
        send(PAIR, (PAIR, s), part, tokens.at[q, 1, :, columns(quarter)], (other, j))

    onwards = {}
    for s in range(1, chips):
        for k in range(tp_count):
            told = [onward_of(n, s)[1 if k < PLANE else 2] for n in range(chips)]
            if any(told):
                onward = pick([onward_of(n, s)[0] for n in range(chips)])
                onwards[s, k] = (onward, pick([int(t) for t in told]) > 0)

    def onward_send(s, k):
        q = sources[s]
        part = tokens.at[q, 0, :, columns(quarters[k])]
        if (s, k) in onwards:
            onward, more = onwards[s, k]
            device = (onward * CORES + c, j)
            send((ONWARD, s, k - k % PLANE), (), part, part, device, line_recv.at[q, k], more)

    def cross_arrival(s, k):
        q = sources[s]
        part = tokens.at[q, 0, :, columns(quarters[k])]
        arrive((CROSS, s, k - PLANE), part)
        onward_send(s, k)
        send(PAIR, (PAIR, s), part, tokens.at[q, 1, :, columns(quarters[k])], (other, j))

    def expert_up(s):
        q = sources[s]
        arrive((ROUTE, s), route.at[q, 1])
        if s == 0:
            loaded(gate_load, up_load)
        for p in range(CORES):
            picks, _ = choice(s, p)
            if p == 1:
                arrive((PAIR, s), tokens.at[q, 1])
            rows_in[p * capacity : (p + 1) * capacity, :] = dot(
                picks.astype(bf16), tokens[q, p]
            ).astype(bf16)
        held = silu(dot(rows_in[...], gate_v[...])) * dot(rows_in[...], up_v[...])
        hidden[q, :, columns(j)] = held.astype(bf16)

    def up_part(s, t):
        q = sources[s]
        p = (t + c) % CORES
        if t == 0:
            arrive((ROUTE, s), route.at[q, 1])
            arrive((PAIR, s), tokens.at[q, 1])
        picks, _ = choice(s, p)
        taken = dot(picks.astype(bf16), tokens[q, p]).astype(bf16)
        held = silu(dot(taken, gate_v[...])) * dot(taken, up_v[...])
        hidden[q, t * capacity : (t + 1) * capacity, columns(j)] = held.astype(bf16)

    def part_ref(s, t):
        return hidden.at[sources[s], pl.ds(t * capacity, capacity)]

    def down_part(s, t):
        q = sources[s]
        gather_finish((HIDDEN, s, t), part_ref(s, t))
        picks, weight = choice(s, (t + c) % CORES)
        full = dot(hidden[q, t * capacity : (t + 1) * capacity], down_v[...])
        scale = jnp.sum(picks * weight, axis=1, keepdims=True)
        scaled = (full * scale).astype(bf16)
        spread = lax.dot_general(
            picks.astype(bf16), scaled, (((0,), (0,)), ((), ())), preferred_element_type=f32
        ).astype(bf16)

        @pl.when(c == t)
        def _():
            sent_sum[q] = spread

        @pl.when(c != t)
        def _():
            own_part[q] = spread
            send(PART, (PART, s), own_part.at[q], peer_part.at[q], (other, j))

    def return_part(s, t):
        @pl.when(c == t)
        def _():
            expert_return(s)

    def start_x(s):
        gather_x((HIDDEN, s), hidden.at[sources[s]])

    def start_y(s):
        gather_y((HIDDEN, s), hidden.at[sources[s]])

    def start(s):
        start_x(s)
        start_y(s)

    def relay(s):
        relay_x((HIDDEN, s), hidden.at[sources[s]])
        relay_y((HIDDEN, s), hidden.at[sources[s]])

    def start_part(s, t):
        gather_x((HIDDEN, s, t), part_ref(s, t))
        gather_y((HIDDEN, s, t), part_ref(s, t))

    def relay_part(s, t):
        relay_x((HIDDEN, s, t), part_ref(s, t))
        relay_y((HIDDEN, s, t), part_ref(s, t))

    def collect(s):
        q = sources[s]
        arrive((), returned.at[q], return_recv.at[q])
        total_ref[...] = total_ref[...] + returned[q].astype(f32)

    def expert_down(s):
        q = sources[s]
        gather_finish((HIDDEN, s), hidden.at[q])
        full = dot(hidden[q], down_v[...])
        for p in reversed(range(CORES)):
            picks, weight = choice(s, p)
            scale = jnp.sum(picks * weight, axis=1, keepdims=True)
            scaled = (full[p * capacity : (p + 1) * capacity] * scale).astype(bf16)
            spread = lax.dot_general(
                picks.astype(bf16), scaled, (((0,), (0,)), ((), ())), preferred_element_type=f32
            )
            if p == 1:
                own_part[q] = spread.astype(bf16)
                send(PART, (PART, s), own_part.at[q], peer_part.at[q], (other, j))
            elif s == 0:
                total_ref[...] = total_ref[...] + spread
            else:
                sent_sum[q] = spread.astype(bf16)

    def expert_return(s):
        q = sources[s]
        arrive((PART, s), peer_part.at[q])
        if s == 0:
            total_ref[...] = total_ref[...] + peer_part[q].astype(f32)
        else:
            sent_sum[q] = (sent_sum[q].astype(f32) + peer_part[q].astype(f32)).astype(bf16)
            send(RETURN, (), sent_sum.at[q], returned.at[z], (q * CORES + c, j), return_recv.at[z])

    def stats_start(k, values):
        lane = lax.broadcasted_iota(jnp.int32, (rows, rows), 1)
        total = jnp.sum(values, axis=1, keepdims=True)
        square = jnp.sum(values * values, axis=1, keepdims=True)
        tile = jnp.where(lane == 0, total, jnp.where(lane == 1, square, 0.0))
        stats_out[k] = tile.T[0 : stats_out.shape[1], :]
        for n, peer in enumerate((jx, jy, jd)):
            send((STATS, k), (STATS, k), stats_out.at[k], stats_in.at[k, n], (me, peer))

    def stats_finish(k, values, gain_ref, bias_ref, out_ref):
        tile = stats_out[k]
        arrive((STATS, k), stats_in.at[k])
        for n in range(tp_count - 1):
            tile = tile + stats_in[k, n]
        padded = jnp.concatenate(
            [tile, jnp.zeros((rows - tile.shape[0], rows), f32)], axis=0
        ).T
        average = padded[:, 0:1] / full_width
        spread = padded[:, 1:2] / full_width - average * average
        scaled = (values - average) * lax.rsqrt(spread + 1e-05)
        out_ref[...] = (
            scaled * gain_ref[...].astype(f32).reshape(1, cols)
            + bias_ref[...].astype(f32).reshape(1, cols)
        ).astype(bf16)

    def shared_start():
        loaded(shared_gate_load, shared_up_load)
        own = tokens[z, 0]
        held = silu(dot(own, shared_gate_v[...])) * dot(own, shared_up_v[...])
        shared_hidden[:, columns(j)] = held.astype(bf16)
        gather_x((SHARED,), shared_hidden)
        gather_y((SHARED,), shared_hidden)

    def mixer_start():
        pl.when(me > 0)(lambda: arrive(EDGE, border))
        loaded(outer_load, taps_load)
        extended[pad - edge_rows : pad, :] = border[...].astype(f32)
        places = (me * rows + lax.broadcasted_iota(jnp.int32, (rows, 1), 0)) % seq_length
        taps_count = taps_ref.shape[0]
        convolved = jnp.zeros((rows, cols), f32)
        for offset in range(taps_count):
            delay = taps_count - 1 - offset
            delayed = extended[pad - delay : pad - delay + rows, :]
            kept = (places >= delay).astype(f32)
            convolved = convolved + taps_ref[offset : offset + 1, :].astype(f32) * delayed * kept
        weighted[:, columns(j)] = (outer_ref[...].astype(f32) * convolved).astype(bf16)
        gather_x((MIXER,), weighted)
        gather_y((MIXER,), weighted)

    def shared_relay():
        relay_x((SHARED,), shared_hidden)
        relay_y((SHARED,), shared_hidden)

    def mixer_relay():
        relay_x((MIXER,), weighted)
        relay_y((MIXER,), weighted)

    def mixer_dot():
        gather_finish((MIXER,), weighted)
        loaded(mix_load)
        mixed_ref[...] = dot(weighted[...], mix_v[...])
        stats_start(0, mixed_ref[...])

    def mixer_end():
        loaded(gain_m_load, bias_m_load, gain_e_load, bias_e_load)
        stats_finish(0, mixed_ref[...], gain_m_ref, bias_m_ref, out_m_ref)

    def shared_dot():
        gather_finish((SHARED,), shared_hidden)
        loaded(shared_down_load, down_load)
        total_ref[...] = dot(shared_hidden[...], shared_down_v[...])

    act = types.SimpleNamespace(
        shared=shared_start,
        up=expert_up,
        start=start,
        start_x=start_x,
        start_y=start_y,
        line=line_arrival,
        cross=cross_arrival,
        relay=relay,
        down=expert_down,
        give_back=expert_return,
        up_part=up_part,
        start_part=start_part,
        relay_part=relay_part,
        down_part=down_part,
        give_back_part=return_part,
        shared_relay=shared_relay,
        shared_dot=shared_dot,
        mixer=mixer_start,
        mixer_relay=mixer_relay,
        mixer_dot=mixer_dot,
        collect=collect,
    )
    inner = (z > 0) & (z < chips - 1)
    for where, step, which in plan(act):
        if where == ALL:
            step(*which)
        else:
            pl.when(inner if where == INNER else ~inner)(functools.partial(step, *which))
    with jax.named_scope("stats"):
        stats_start(1, total_ref[...])
    with jax.named_scope("mixer_end"):
        mixer_end()
    with jax.named_scope("drain"):
        lines = tokens.at[0, 0, :, pl.ds(0, PLANE * cols)]
        sent((UP, 0), lines, higher)
        sent((DOWN, 0), lines, lower)
        sent((UP, PLANE), lines, rising)
        sent((DOWN, PLANE), lines, falling)
        for s, k in onwards:
            if k % PLANE == 0:
                sent((ONWARD, s, k), lines, onwards[s, k][1])
            if k == 0:
                sent((ROUTE, s), route.at[0, 0], onwards[s, k][1])
        sent(ROUTE_UP, route.at[0, 0], higher)
        sent(ROUTE_DOWN, route.at[0, 0], lower)
        sent(PAIR, tokens.at[:, 0])
        sent(ROUTE, route.at[:, 0])
        sent(EDGE, edge, ~last)
        sent((CROSS, 1), lines)
        sent((CROSS, 2), lines, ~inner)
        gathered = pl.ds(0, (tp_count - 1) * cols)
        sent(HIDDEN, hidden.at[:, :, gathered])
        sent(SHARED, shared_hidden.at[:, gathered])
        sent(MIXER, weighted.at[:, gathered])
        sent(PART, own_part)
        sent(RETURN, own_part.at[pl.ds(0, chips - 1)])
        sent((STATS, 0), stats_in.at[0])
    with jax.named_scope("finish"):
        stats_finish(1, total_ref[...], gain_e_ref, bias_e_ref, out_e_ref)
    with jax.named_scope("sent"):
        sent((STATS, 1), stats_in.at[1])


def pass_kernel(first_ref, second_ref, out_first_ref, out_second_ref):
    out_first_ref[...] = first_ref[...]
    out_second_ref[...] = second_ref[...]


def fused_device(
    outer_gate,
    inner_gate,
    conv_value,
    conv_taps,
    mix_out,
    gain_mixer,
    bias_mixer,
    moe_input,
    route_ids,
    route_weights,
    expert_gate,
    expert_up,
    expert_down,
    shared_gate,
    shared_up,
    shared_down,
    gain_experts,
    bias_experts,
):
    rows, cols = outer_gate.shape
    width = moe_input.shape[1]
    ep_count = lax.axis_size("ep")
    tp_count = lax.axis_size("tp")
    chips = ep_count // CORES
    capacity = max(2, 3 * rows * route_ids.shape[1] // (2 * ep_count))
    seq_length = rows * ep_count // SEQS
    bf16, f32 = jnp.bfloat16, jnp.float32
    vmem = pl.BlockSpec(memory_space=pltpu.VMEM)
    hbm = pl.BlockSpec(memory_space=pl.ANY)
    copies = 5 * chips + 20
    weight = pltpu.VMEM((width, cols), bf16)
    scratch = [
        *([pltpu.VMEM((rows, cols), bf16)] * 3),
        pltpu.VMEM(conv_taps.shape, bf16),
        pltpu.VMEM(route_ids.shape[::-1], jnp.int32),
        pltpu.VMEM(route_weights.shape[::-1], f32),
        *([pltpu.VMEM((cols,), bf16)] * 4),
        *([weight] * 7),
        pltpu.VMEM((chips, CORES, rows, width), bf16),
        pltpu.VMEM((chips, CORES, ep_count, rows), f32),
        pltpu.VMEM((CORES * capacity, width), bf16),
        pltpu.VMEM((chips, CORES * capacity, width), bf16),
        pltpu.VMEM((rows, width), bf16),
        pltpu.VMEM((rows, width), bf16),
        pltpu.VMEM((16, cols), bf16),
        pltpu.VMEM((16, cols), bf16),
        pltpu.VMEM((rows + 16, cols), f32),
        pltpu.VMEM((chips, rows, cols), bf16),
        pltpu.VMEM((chips, rows, cols), bf16),
        pltpu.VMEM((chips, rows, cols), bf16),
        pltpu.VMEM((chips, rows, cols), bf16),
        pltpu.VMEM((2, 8, rows), f32),
        pltpu.VMEM((2, tp_count - 1, 8, rows), f32),
        pltpu.VMEM((rows, cols), f32),
        pltpu.VMEM((rows, cols), f32),
        pltpu.SemaphoreType.DMA((18,)),
        pltpu.SemaphoreType.DMA((chips + 22,)),
        pltpu.SemaphoreType.DMA((copies,)),
        pltpu.SemaphoreType.DMA((chips, tp_count)),
        pltpu.SemaphoreType.DMA((chips,)),
        pltpu.SemaphoreType.DMA((chips,)),
    ]
    out = jax.ShapeDtypeStruct((rows, cols), bf16)
    near = pltpu.VMEM((rows, cols), bf16)
    given = (
        outer_gate,
        inner_gate,
        conv_value,
        conv_taps,
        mix_out,
        gain_mixer,
        bias_mixer,
        moe_input,
        route_ids.T,
        route_weights.T,
        expert_gate,
        expert_up,
        expert_down,
        shared_gate,
        shared_up,
        shared_down,
        gain_experts,
        bias_experts,
    )
    first, second = pl.pallas_call(
        functools.partial(fused_kernel, (ep_count, tp_count, capacity, seq_length)),
        out_shape=(near, near),
        in_specs=[hbm] * 18,
        out_specs=(vmem, vmem),
        scratch_shapes=scratch,
        compiler_params=pltpu.CompilerParams(
            collective_id=0, has_side_effects=True, vmem_limit_bytes=VMEM_BYTES
        ),
    )(*(pltpu.with_memory_space_constraint(one, pltpu.HBM) for one in given))
    return pl.pallas_call(
        pass_kernel,
        out_shape=(out, out),
        in_specs=[vmem, vmem],
        out_specs=(vmem, vmem),
        compiler_params=pltpu.CompilerParams(vmem_limit_bytes=SMALL_BYTES),

    )(first, second)


def on_device(*arrays):
    local_experts = arrays[10].shape[0]
    square = lax.axis_size("tp") == PLANE * PLANE
    if square and local_experts == 1 and lax.axis_size("ep") == CORES * LINE:
        return fused_device(*arrays)
    return plain_device(*arrays)


def solution(mesh):
    in_specs = (
        P("ep", "tp"),
        P("ep", "tp"),
        P("ep", "tp"),
        P(None, "tp"),
        P(None, "tp"),
        P("tp"),
        P("tp"),
        P("ep", None),
        P("ep", None),
        P("ep", None),
        P("ep", None, "tp"),
        P("ep", None, "tp"),
        P("ep", None, "tp"),
        P(None, "tp"),
        P(None, "tp"),
        P(None, "tp"),
        P("tp"),
        P("tp"),
    )
    out_specs = (P("ep", "tp"), P("ep", "tp"))
    return jax.shard_map(
        on_device, mesh=mesh, in_specs=in_specs, out_specs=out_specs, check_vma=False
    )
```

```python
import functools
import types

import jax
import jax.numpy as jnp
from jax import lax
from jax.experimental import pallas as pl
from jax.experimental.pallas import tpu as pltpu
from jax.sharding import PartitionSpec as P

SEQS = 1


def shifted(block, axis, distance):
    devices = range(lax.axis_size(axis))
    route = [(i - distance, i) for i in devices if i - distance in devices]
    return lax.ppermute(block, axis, route)


def finish(values, totals, squares, full_width, gain, offset_bias):
    average = (totals / full_width)[:, None]
    spread = (squares / full_width)[:, None] - average * average
    scaled = (values - average) * lax.rsqrt(spread + 1e-05)
    return (scaled * gain.astype(jnp.float32) + offset_bias.astype(jnp.float32)).astype(
        jnp.bfloat16
    )


def plain_device(
    outer_gate,
    inner_gate,
    conv_value,
    conv_taps,
    mix_out,
    gain_mixer,
    bias_mixer,
    moe_input,
    route_ids,
    route_weights,
    expert_gate,
    expert_up,
    expert_down,
    shared_gate,
    shared_up,
    shared_down,
    gain_experts,
    bias_experts,
):
    token_rows = outer_gate.shape[0]
    column_count = outer_gate.shape[1]
    ep_count = lax.axis_size("ep")
    tp_count = lax.axis_size("tp")
    taps_count = conv_taps.shape[0]
    product = (inner_gate.astype(jnp.float32) * conv_value.astype(jnp.float32)).astype(jnp.bfloat16)
    border = shifted(product[token_rows - (taps_count - 1) :], "ep", 1)
    extended = jnp.concatenate([border, product], axis=0).astype(jnp.float32)
    seq_length = token_rows * ep_count // SEQS
    places = (
        lax.axis_index("ep") * token_rows + jnp.arange(token_rows, dtype=jnp.int32)
    ) % seq_length
    convolved = jnp.zeros((token_rows, column_count), jnp.float32)
    for offset in range(taps_count):
        delay_rows = taps_count - 1 - offset
        delayed = extended[offset : offset + token_rows]
        kept_mask = (places >= delay_rows).astype(jnp.float32)[:, None]
        convolved = convolved + conv_taps[offset].astype(jnp.float32)[None, :] * delayed * kept_mask
    weighted_in = (outer_gate.astype(jnp.float32) * convolved).astype(jnp.bfloat16)
    block = mix_out
    mixed = jnp.dot(
        lax.all_gather(weighted_in, "tp", axis=1, tiled=True),
        block,
        preferred_element_type=jnp.float32,
    )
    topk_count = route_ids.shape[1]
    local_experts = expert_gate.shape[0]
    expert_count = local_experts * ep_count
    capacity = max(2, 3 * token_rows * topk_count // (2 * expert_count))
    flat_ids = route_ids.reshape(-1)
    marks = (flat_ids[:, None] == jnp.arange(expert_count, dtype=jnp.int32)[None, :]).astype(
        jnp.int32
    )
    ranks = jnp.sum((jnp.cumsum(marks, axis=0) - marks) * marks, axis=1)
    targets = flat_ids * capacity + ranks
    sources = jnp.arange(flat_ids.shape[0], dtype=jnp.int32) // topk_count
    sent_rows = lax.dynamic_slice_in_dim(
        moe_input, lax.axis_index("tp") * column_count, column_count, 1
    )
    buffer_rows = jnp.zeros((expert_count * capacity, sent_rows.shape[1]), jnp.bfloat16)
    buffer_rows = buffer_rows.at[targets].set(sent_rows[sources])
    sectioned = buffer_rows.reshape(ep_count, local_experts * capacity, sent_rows.shape[1])
    arrived = lax.all_to_all(sectioned, "ep", split_axis=0, concat_axis=0, tiled=True)
    arrived = lax.all_gather(arrived, "tp", axis=2, tiled=True)
    expert_rows = arrived.reshape(ep_count, local_experts, capacity, arrived.shape[2])
    gate_value = jnp.einsum(
        "secd,edf->secf", expert_rows, expert_gate, preferred_element_type=jnp.float32
    )
    up_value = jnp.einsum(
        "secd,edf->secf", expert_rows, expert_up, preferred_element_type=jnp.float32
    )
    hidden = (jax.nn.silu(gate_value) * up_value).astype(jnp.bfloat16)
    flat_hidden = hidden.reshape(expert_count * capacity, hidden.shape[3])
    shared_gate_value = jnp.dot(moe_input, shared_gate, preferred_element_type=jnp.float32)
    shared_up_value = jnp.dot(moe_input, shared_up, preferred_element_type=jnp.float32)
    shared_hidden = (jax.nn.silu(shared_gate_value) * shared_up_value).astype(jnp.bfloat16)
    piece = lax.all_gather(flat_hidden, "tp", axis=1, tiled=True)
    block = expert_down
    shaped = piece.reshape(ep_count, local_experts, capacity, piece.shape[1])
    routed_sum = jnp.einsum("secf,efd->secd", shaped, block, preferred_element_type=jnp.float32)
    block = shared_down
    shared_sum = jnp.dot(
        lax.all_gather(shared_hidden, "tp", axis=1, tiled=True),
        block,
        preferred_element_type=jnp.float32,
    )
    expert_out = routed_sum.astype(jnp.bfloat16).reshape(
        ep_count, local_experts * capacity, column_count
    )
    returned = lax.all_to_all(expert_out, "ep", split_axis=0, concat_axis=0, tiled=True)
    picked = returned.reshape(expert_count * capacity, column_count)[targets].astype(jnp.float32)
    weighted = picked.reshape(token_rows, topk_count, column_count) * route_weights[:, :, None]
    combined = jnp.sum(weighted, axis=1) + shared_sum
    mixer_total, mixer_square, expert_total, expert_square = lax.psum(
        (
            jnp.sum(mixed, axis=1),
            jnp.sum(mixed * mixed, axis=1),
            jnp.sum(combined, axis=1),
            jnp.sum(combined * combined, axis=1),
        ),
        "tp",
    )
    full_width = column_count * tp_count
    out_mixer = finish(mixed, mixer_total, mixer_square, full_width, gain_mixer, bias_mixer)
    out_experts = finish(
        combined, expert_total, expert_square, full_width, gain_experts, bias_experts
    )
    return (out_mixer, out_experts)


PLANE = 2
SMALL_BYTES = 4 * 1024 * 1024
CORES = 2
VMEM_BYTES = 48 * 1024 * 1024


(
    UP,
    DOWN,
    ROUTE,
    PAIR,
    EDGE,
    CROSS,
    HIDDEN,
    SHARED,
    MIXER,
    PART,
    RETURN,
    STATS,
    ONWARD,
    ROUTE_UP,
    ROUTE_DOWN,
) = range(15)
LINE = 4
ALL, INNER, OUTER = range(3)


def plan(act):
    return [
        (ALL, act.shared, ()),
        (ALL, act.up, (0,)),
        (ALL, act.start_y, (0,)),
        (ALL, act.start_x, (0, 0)),
        (ALL, act.line, (1, 0, True)),
        (INNER, act.line, (2, 0)),
        (ALL, act.start_x, (0, 1)),
        (ALL, act.line, (1, 1, True)),
        (INNER, act.line, (2, 1)),
        (ALL, act.shared_relay, ()),
        (OUTER, act.line, (2, 0, True)),
        (INNER, act.line, (2, 2)),
        (INNER, act.line, (3, 0)),
        (ALL, act.cross, (1, 2)),
        (ALL, act.cross, (1, 3)),
        (INNER, act.line, (2, 3)),
        (OUTER, act.line, (2, 1, True)),
        (INNER, act.line, (3, 1)),
        (ALL, act.up, (1,)),
        (ALL, act.start, (1,)),
        (INNER, act.line, (3, 2)),
        (OUTER, act.line, (3, 0)),
        (OUTER, act.cross, (2, 2)),
        (OUTER, act.cross, (2, 3)),
        (OUTER, act.line, (3, 1)),
        (OUTER, act.relay, (0,)),
        (ALL, act.up, (2,)),
        (ALL, act.start, (2,)),
        (INNER, act.line, (3, 3)),
        (ALL, act.shared_dot, ()),
        (OUTER, act.line, (3, 2)),
        (OUTER, act.line, (3, 3)),
        (INNER, act.relay, (1,)),
        (ALL, act.up_part, (3, 0)),
        (ALL, act.start_part, (3, 0)),
        (INNER, act.relay, (2,)),
        (ALL, act.up_part, (3, 1)),
        (ALL, act.start_part, (3, 1)),
        (INNER, act.down, (1,)),
        (INNER, act.give_back, (1,)),
        (ALL, act.relay_part, (3, 0)),
        (INNER, act.down, (2,)),
        (ALL, act.relay_part, (3, 1)),
        (INNER, act.give_back, (2,)),
        (OUTER, act.relay, (2,)),
        (OUTER, act.relay, (1,)),
        (ALL, act.mixer, ()),
        (INNER, act.relay, (0,)),
        (ALL, act.down_part, (3, 0)),
        (ALL, act.give_back_part, (3, 0)),
        (ALL, act.down_part, (3, 1)),
        (ALL, act.give_back_part, (3, 1)),
        (OUTER, act.down, (2,)),
        (OUTER, act.give_back, (2,)),
        (OUTER, act.down, (1,)),
        (ALL, act.mixer_relay, (0,)),
        (OUTER, act.give_back, (1,)),
        (ALL, act.mixer_relay, (1,)),
        (ALL, act.down, (0,)),
        (ALL, act.give_back, (0,)),
        (ALL, act.mixer_dot, ()),
        (ALL, act.collect, (1,)),
        (ALL, act.collect, (2,)),
        (ALL, act.collect, (3,)),
    ]


def nearest_first(chips):
    def key(z):
        return lambda k: (abs(k - z), abs(2 * k - (chips - 1)))

    return [sorted((k for k in range(chips) if k != z), key=key(z)) for z in range(chips)]


def silu(value):
    return value / (1.0 + jnp.exp(-value))


def fused_kernel(
    shape,
    outer_hbm,
    inner_hbm,
    value_hbm,
    taps_hbm,
    mix_hbm,
    gain_m_hbm,
    bias_m_hbm,
    moe_hbm,
    ids_hbm,
    route_w_hbm,
    gate_hbm,
    up_hbm,
    down_hbm,
    shared_gate_hbm,
    shared_up_hbm,
    shared_down_hbm,
    gain_e_hbm,
    bias_e_hbm,
    out_m_ref,
    out_e_ref,
    outer_ref,
    inner_ref,
    value_ref,
    taps_ref,
    ids_ref,
    route_w_ref,
    gain_m_ref,
    bias_m_ref,
    gain_e_ref,
    bias_e_ref,
    mix_v,
    gate_v,
    up_v,
    down_v,
    shared_gate_v,
    shared_up_v,
    shared_down_v,
    tokens,
    route,
    rows_in,
    hidden,
    weighted,
    shared_hidden,
    border,
    edge,
    extended,
    peer_part,
    own_part,
    sent_sum,
    returned,
    stats_out,
    stats_in,
    mixed_ref,
    total_ref,
    load_sem,
    send_sem,
    recv_sem,
    line_recv,
    route_recv,
    return_recv,
):
    ep_count, tp_count, capacity, seq_length = shape
    chips = ep_count // CORES
    rows, cols = outer_ref.shape
    full_width = cols * tp_count
    me = lax.axis_index("ep")
    j = lax.axis_index("tp")
    z = me // CORES
    c = me % CORES
    x = j % PLANE
    y = j // PLANE
    jx = y * PLANE + (1 - x)
    jy = (1 - y) * PLANE + x
    jd = (1 - y) * PLANE + (1 - x)
    other = z * CORES + (1 - c)
    f32, bf16 = jnp.float32, jnp.bfloat16

    orders = nearest_first(chips)

    def pick(values):
        chosen = jnp.int32(values[0])
        for k in range(1, chips):
            chosen = jnp.where(z == k, values[k], chosen)
        return chosen

    sources = [z] + [pick([orders[k][s - 1] for k in range(chips)]) for s in range(1, chips)]

    def whole(k, q):
        s = orders[k].index(q) + 1
        return s == chips - 1 or s == chips - 2 and 0 < k < chips - 1

    def onward_of(k, s):
        q = orders[k][s - 1]
        n = k + 1 if q < k else k - 1
        there = 0 <= n < chips
        return n if there else k, there, there and whole(n, q)

    rising = pick([int(k + 1 < chips and whole(k + 1, k)) for k in range(chips)]) > 0
    falling = pick([int(k > 0 and whole(k - 1, k)) for k in range(chips)]) > 0

    loads = []

    def load(source, target):
        loads.append(pltpu.make_async_copy(source, target, load_sem.at[len(loads)]))
        loads[-1].start()
        return loads[-1]

    above = (z + 1) % chips
    below = (z + chips - 1) % chips
    higher = z + 1 < chips
    lower = z > 0
    beside = jnp.where(c > 0, me + 1, me + ep_count - 1) % ep_count
    slanted = jnp.where(c > 0, z + 1 < chips, z > 0)

    barrier = pltpu.get_barrier_semaphore()

    def greet(row, column):
        pl.semaphore_signal(
            barrier, inc=1, device_id=(row, column), device_id_type=pl.DeviceIdType.MESH
        )

    greet(other, j)
    greet(me, jx)
    greet(me, jy)
    pl.when(higher)(lambda: greet(above * CORES + c, j))
    pl.when(lower)(lambda: greet(below * CORES + c, j))
    pl.when(slanted)(lambda: greet(beside, j))
    greeted = 3 + higher.astype(jnp.int32) + lower.astype(jnp.int32) + slanted.astype(jnp.int32)

    moe_load = load(moe_hbm, tokens.at[z, 0])
    ids_load = load(ids_hbm, ids_ref)
    route_w_load = load(route_w_hbm, route_w_ref)
    inner_load = load(inner_hbm, inner_ref)
    value_load = load(value_hbm, value_ref)
    shared_gate_load = load(shared_gate_hbm, shared_gate_v)
    shared_up_load = load(shared_up_hbm, shared_up_v)
    gate_load = load(gate_hbm.at[0], gate_v)
    up_load = load(up_hbm.at[0], up_v)
    outer_load = load(outer_hbm, outer_ref)
    taps_load = load(taps_hbm, taps_ref)
    gain_m_load = load(gain_m_hbm, gain_m_ref)
    bias_m_load = load(bias_m_hbm, bias_m_ref)
    gain_e_load = load(gain_e_hbm, gain_e_ref)
    bias_e_load = load(bias_e_hbm, bias_e_ref)
    shared_down_load = load(shared_down_hbm, shared_down_v)
    down_load = load(down_hbm.at[0], down_v)
    mix_load = load(mix_hbm, mix_v)

    def loaded(*several):
        for one in several:
            one.wait()

    loaded(moe_load)
    with jax.named_scope("barrier"):
        pl.semaphore_wait(barrier, greeted)

    groups = {}
    numbers = {}

    def remote(source, target, sent, received, device):
        return pltpu.make_async_remote_copy(
            src_ref=source,
            dst_ref=target,
            send_sem=sent,
            recv_sem=received,
            device_id=device,
            device_id_type=pl.DeviceIdType.MESH,
        )

    def group(name):
        return send_sem.at[groups.setdefault(name, len(groups))]

    def number(name):
        return recv_sem.at[numbers.setdefault(name, len(numbers))]

    def send(many, name, source, target, device, received=None, when=None):
        copy = remote(source, target, group(many), number(name) if received is None else received, device)
        if when is None:
            copy.start()
        else:
            pl.when(when)(copy.start)

    def arrive(name, target, received=None):
        remote(target, target, group(EDGE), number(name) if received is None else received, (other, j)).wait_recv()

    def sent(many, ref, when=None):
        def wait():
            remote(ref, ref, group(many), number(EDGE), (other, j)).wait_send()

        if when is None:
            wait()
        else:
            pl.when(when)(wait)

    def columns(owner):
        return pl.ds(pl.multiple_of(owner * cols, cols), cols)

    def gather_x(name, ref):
        part = ref.at[:, columns(j)]
        send(name[0], name + (0,), part, part, (me, jx))

    def gather_y(name, ref):
        part = ref.at[:, columns(j)]
        send(name[0], name + (1,), part, part, (me, jy))

    def relay_x(name, ref):
        half = ref.shape[0] // 2
        arrive(name + (0,), ref.at[:, columns(jx)])
        part = ref.at[pl.ds(0, half), columns(jx)]
        send(name[0], name + (2,), part, part, (me, jy))

    def relay_y(name, ref):
        half = ref.shape[0] // 2
        arrive(name + (1,), ref.at[:, columns(jy)])
        part = ref.at[pl.ds(half, half), columns(jy)]
        send(name[0], name + (2,), part, part, (me, jx))

    def gather_finish(name, ref):
        arrive(name + (2,), ref.at[:, columns(jd)])

    quarters = (x, PLANE + y, 1 - x, PLANE + 1 - y)
    def line_start(k):
        part = tokens.at[z, 0, :, columns(quarters[k])]
        received = line_recv.at[z, k]
        more = k - k % PLANE
        device = (above * CORES + c, j)
        send((UP, more), (), part, part, device, received, rising if more else higher)
        device = (below * CORES + c, j)
        send((DOWN, more), (), part, part, device, received, falling if more else lower)

    line_start(0)
    send(PAIR, (PAIR, 0), tokens.at[z, 0], tokens.at[z, 1], (other, j))
    loaded(ids_load, route_w_load)
    named = lax.broadcasted_iota(jnp.int32, (ep_count, rows), 0)
    dense = jnp.zeros((ep_count, rows), f32)
    for k in range(ids_ref.shape[0]):
        dense = dense + jnp.where(named == ids_ref[k : k + 1, :], route_w_ref[k : k + 1, :], 0.0)
    route[z, 0] = dense
    own = route.at[z, 0]
    send(ROUTE_UP, (), own, own, (above * CORES + c, j), route_recv.at[z], higher)
    send(ROUTE_DOWN, (), own, own, (below * CORES + c, j), route_recv.at[z], lower)
    send(ROUTE, (ROUTE, 0), own, route.at[z, 1], (other, j))
    line_start(1)
    line_start(2)
    line_start(3)
    loaded(inner_load, value_load)
    product = (inner_ref[...].astype(f32) * value_ref[...].astype(f32)).astype(bf16)
    edge_rows = edge.shape[0]
    edge[...] = product[rows - edge_rows :]

    @pl.when(me == 0)
    def _():
        border[...] = jnp.zeros_like(border)

    pad = extended.shape[0] - rows
    extended[pad:, :] = product.astype(f32)
    last = me == ep_count - 1
    send(EDGE, EDGE, edge, border, ((me + 1) % ep_count, j), None, ~last)

    def dot(a, b):
        return jnp.dot(a, b, preferred_element_type=f32)

    def choice(s, p):
        weight = route[sources[s], p, pl.ds(me, 1), :]
        routed = (weight > 0.0).astype(f32)
        earlier = lax.broadcasted_iota(jnp.int32, (rows, rows), 0)
        later = lax.broadcasted_iota(jnp.int32, (rows, rows), 1)
        upper = (earlier <= later).astype(f32).astype(bf16)
        many = jnp.broadcast_to(routed, (16, rows)).astype(bf16)
        rank = dot(many, upper)[0:1, :] * routed
        slot = lax.broadcasted_iota(jnp.int32, (capacity, rows), 0).astype(f32) + 1.0
        return (slot == rank).astype(f32), weight

    def line_arrival(s, k, swap=False):
        q = sources[s]
        quarter = quarters[k]
        part = tokens.at[q, 0, :, columns(quarter)]
        if k == 1:
            own = route.at[q, 0]
            arrive((), own, route_recv.at[q])
            if (s, k) in onwards:
                onward, more = onwards[s, k]
                device = (onward * CORES + c, j)
                send((ROUTE, s), (), own, own, device, route_recv.at[q], more)
            send(ROUTE, (ROUTE, s), own, route.at[q, 1], (other, j))
        arrive((), part, line_recv.at[q, k])
        onward_send(s, k)
        if swap:
            send((CROSS, s), (CROSS, s, k), part, part, (me, (jx, jy)[k]))
        send(PAIR, (PAIR, s), part, tokens.at[q, 1, :, columns(quarter)], (other, j))

    onwards = {}
    for s in range(1, chips):
        for k in range(tp_count):
            told = [onward_of(n, s)[1 if k < PLANE else 2] for n in range(chips)]
            if any(told):
                onward = pick([onward_of(n, s)[0] for n in range(chips)])
                onwards[s, k] = (onward, pick([int(t) for t in told]) > 0)

    def onward_send(s, k):
        q = sources[s]
        part = tokens.at[q, 0, :, columns(quarters[k])]
        if (s, k) in onwards:
            onward, more = onwards[s, k]
            device = (onward * CORES + c, j)
            send((ONWARD, s, k - k % PLANE), (), part, part, device, line_recv.at[q, k], more)

    def cross_arrival(s, k):
        q = sources[s]
        part = tokens.at[q, 0, :, columns(quarters[k])]
        arrive((CROSS, s, k - PLANE), part)
        onward_send(s, k)
        send(PAIR, (PAIR, s), part, tokens.at[q, 1, :, columns(quarters[k])], (other, j))

    def expert_up(s):
        q = sources[s]
        arrive((ROUTE, s), route.at[q, 1])
        if s == 0:
            loaded(gate_load, up_load)
        for p in range(CORES):
            picks, _ = choice(s, p)
            if p == 1:
                arrive((PAIR, s), tokens.at[q, 1])
            rows_in[p * capacity : (p + 1) * capacity, :] = dot(
                picks.astype(bf16), tokens[q, p]
            ).astype(bf16)
        held = silu(dot(rows_in[...], gate_v[...])) * dot(rows_in[...], up_v[...])
        hidden[q, :, columns(j)] = held.astype(bf16)

    def up_part(s, t):
        q = sources[s]
        p = (t + c) % CORES
        if t == 0:
            arrive((ROUTE, s), route.at[q, 1])
            arrive((PAIR, s), tokens.at[q, 1])
        picks, _ = choice(s, p)
        taken = dot(picks.astype(bf16), tokens[q, p]).astype(bf16)
        held = silu(dot(taken, gate_v[...])) * dot(taken, up_v[...])
        hidden[q, t * capacity : (t + 1) * capacity, columns(j)] = held.astype(bf16)

    def part_ref(s, t):
        return hidden.at[sources[s], pl.ds(t * capacity, capacity)]

    def down_part(s, t):
        q = sources[s]
        gather_finish((HIDDEN, s, t), part_ref(s, t))
        picks, weight = choice(s, (t + c) % CORES)
        full = dot(hidden[q, t * capacity : (t + 1) * capacity], down_v[...])
        scale = jnp.sum(picks * weight, axis=1, keepdims=True)
        scaled = (full * scale).astype(bf16)
        spread = lax.dot_general(
            picks.astype(bf16), scaled, (((0,), (0,)), ((), ())), preferred_element_type=f32
        ).astype(bf16)

        @pl.when(c == t)
        def _():
            sent_sum[q] = spread

        @pl.when(c != t)
        def _():
            own_part[q] = spread
            send(PART, (PART, s), own_part.at[q], peer_part.at[q], (other, j))

    def return_part(s, t):
        @pl.when(c == t)
        def _():
            expert_return(s)

    def start_x(s, t=None):
        ref = hidden.at[sources[s]] if t is None else part_ref(s, t)
        gather_x((HIDDEN, s), ref)

    def start_y(s):
        gather_y((HIDDEN, s), hidden.at[sources[s]])

    def start(s):
        start_x(s)
        start_y(s)

    def relay(s):
        relay_x((HIDDEN, s), hidden.at[sources[s]])
        relay_y((HIDDEN, s), hidden.at[sources[s]])

    def start_part(s, t):
        gather_x((HIDDEN, s, t), part_ref(s, t))
        gather_y((HIDDEN, s, t), part_ref(s, t))

    def relay_part(s, t):
        relay_x((HIDDEN, s, t), part_ref(s, t))
        relay_y((HIDDEN, s, t), part_ref(s, t))

    def collect(s):
        q = sources[s]
        arrive((), returned.at[q], return_recv.at[q])
        total_ref[...] = total_ref[...] + returned[q].astype(f32)

    def expert_down(s):
        q = sources[s]
        gather_finish((HIDDEN, s), hidden.at[q])
        full = dot(hidden[q], down_v[...])
        for p in reversed(range(CORES)):
            picks, weight = choice(s, p)
            scale = jnp.sum(picks * weight, axis=1, keepdims=True)
            scaled = (full[p * capacity : (p + 1) * capacity] * scale).astype(bf16)
            spread = lax.dot_general(
                picks.astype(bf16), scaled, (((0,), (0,)), ((), ())), preferred_element_type=f32
            )
            if p == 1:
                own_part[q] = spread.astype(bf16)
                send(PART, (PART, s), own_part.at[q], peer_part.at[q], (other, j))
            elif s == 0:
                total_ref[...] = total_ref[...] + spread
            else:
                sent_sum[q] = spread.astype(bf16)

    def expert_return(s):
        q = sources[s]
        arrive((PART, s), peer_part.at[q])
        if s == 0:
            total_ref[...] = total_ref[...] + peer_part[q].astype(f32)
        else:
            sent_sum[q] = (sent_sum[q].astype(f32) + peer_part[q].astype(f32)).astype(bf16)
            send(RETURN, (), sent_sum.at[q], returned.at[z], (q * CORES + c, j), return_recv.at[z])

    def stats_start(k, values):
        lane = lax.broadcasted_iota(jnp.int32, (rows, rows), 1)
        total = jnp.sum(values, axis=1, keepdims=True)
        square = jnp.sum(values * values, axis=1, keepdims=True)
        tile = jnp.where(lane == 0, total, jnp.where(lane == 1, square, 0.0))
        stats_out[k] = tile.T[0 : stats_out.shape[1], :]
        for n, peer in enumerate((jx, jy, jd)):
            send((STATS, k), (STATS, k), stats_out.at[k], stats_in.at[k, n], (me, peer))

    def stats_finish(k, values, gain_ref, bias_ref, out_ref):
        tile = stats_out[k]
        arrive((STATS, k), stats_in.at[k])
        for n in range(tp_count - 1):
            tile = tile + stats_in[k, n]
        padded = jnp.concatenate(
            [tile, jnp.zeros((rows - tile.shape[0], rows), f32)], axis=0
        ).T
        average = padded[:, 0:1] / full_width
        spread = padded[:, 1:2] / full_width - average * average
        scaled = (values - average) * lax.rsqrt(spread + 1e-05)
        out_ref[...] = (
            scaled * gain_ref[...].astype(f32).reshape(1, cols)
            + bias_ref[...].astype(f32).reshape(1, cols)
        ).astype(bf16)

    def shared_start():
        loaded(shared_gate_load, shared_up_load)
        own = tokens[z, 0]
        held = silu(dot(own, shared_gate_v[...])) * dot(own, shared_up_v[...])
        shared_hidden[:, columns(j)] = held.astype(bf16)
        gather_x((SHARED,), shared_hidden)
        gather_y((SHARED,), shared_hidden)

    def mixer_ref(t):
        return weighted.at[pl.ds(t * (rows // 2), rows // 2)]

    def mixer_start():
        pl.when(me > 0)(lambda: arrive(EDGE, border))
        loaded(outer_load, taps_load)
        extended[pad - edge_rows : pad, :] = border[...].astype(f32)
        places = (me * rows + lax.broadcasted_iota(jnp.int32, (rows, 1), 0)) % seq_length
        taps_count = taps_ref.shape[0]
        convolved = jnp.zeros((rows, cols), f32)
        for offset in range(taps_count):
            delay = taps_count - 1 - offset
            delayed = extended[pad - delay : pad - delay + rows, :]
            kept = (places >= delay).astype(f32)
            convolved = convolved + taps_ref[offset : offset + 1, :].astype(f32) * delayed * kept
        weighted[:, columns(j)] = (outer_ref[...].astype(f32) * convolved).astype(bf16)
        for t in range(2):
            gather_x((MIXER, t), mixer_ref(t))
            gather_y((MIXER, t), mixer_ref(t))

    def shared_relay():
        relay_x((SHARED,), shared_hidden)
        relay_y((SHARED,), shared_hidden)

    def mixer_relay(t):
        relay_x((MIXER, t), mixer_ref(t))
        relay_y((MIXER, t), mixer_ref(t))

    def mixer_dot():
        gather_finish((MIXER, 0), mixer_ref(0))
        gather_finish((MIXER, 1), mixer_ref(1))
        loaded(mix_load)
        mixed_ref[...] = dot(weighted[...], mix_v[...])
        stats_start(0, mixed_ref[...])

    def mixer_end():
        loaded(gain_m_load, bias_m_load, gain_e_load, bias_e_load)
        stats_finish(0, mixed_ref[...], gain_m_ref, bias_m_ref, out_m_ref)

    def shared_dot():
        gather_finish((SHARED,), shared_hidden)
        loaded(shared_down_load, down_load)
        total_ref[...] = dot(shared_hidden[...], shared_down_v[...])

    act = types.SimpleNamespace(
        shared=shared_start,
        up=expert_up,
        start=start,
        start_x=start_x,
        start_y=start_y,
        line=line_arrival,
        cross=cross_arrival,
        relay=relay,
        down=expert_down,
        give_back=expert_return,
        up_part=up_part,
        start_part=start_part,
        relay_part=relay_part,
        down_part=down_part,
        give_back_part=return_part,
        shared_relay=shared_relay,
        shared_dot=shared_dot,
        mixer=mixer_start,
        mixer_relay=mixer_relay,
        mixer_dot=mixer_dot,
        collect=collect,
    )
    inner = (z > 0) & (z < chips - 1)
    for where, step, which in plan(act):
        if where == ALL:
            step(*which)
        else:
            pl.when(inner if where == INNER else ~inner)(functools.partial(step, *which))
    with jax.named_scope("stats"):
        stats_start(1, total_ref[...])
    with jax.named_scope("mixer_end"):
        mixer_end()
    with jax.named_scope("drain"):
        lines = tokens.at[0, 0, :, pl.ds(0, PLANE * cols)]
        sent((UP, 0), lines, higher)
        sent((DOWN, 0), lines, lower)
        sent((UP, PLANE), lines, rising)
        sent((DOWN, PLANE), lines, falling)
        for s, k in onwards:
            if k % PLANE == 0:
                sent((ONWARD, s, k), lines, onwards[s, k][1])
            if k == 0:
                sent((ROUTE, s), route.at[0, 0], onwards[s, k][1])
        sent(ROUTE_UP, route.at[0, 0], higher)
        sent(ROUTE_DOWN, route.at[0, 0], lower)
        sent(PAIR, tokens.at[:, 0])
        sent(ROUTE, route.at[:, 0])
        sent(EDGE, edge, ~last)
        sent((CROSS, 1), lines)
        sent((CROSS, 2), lines, ~inner)
        gathered = pl.ds(0, (tp_count - 1) * cols)
        sent(HIDDEN, hidden.at[:, :, gathered])
        sent(SHARED, shared_hidden.at[:, gathered])
        sent(MIXER, weighted.at[:, gathered])
        sent(PART, own_part)
        sent(RETURN, own_part.at[pl.ds(0, chips - 1)])
        sent((STATS, 0), stats_in.at[0])
    with jax.named_scope("finish"):
        stats_finish(1, total_ref[...], gain_e_ref, bias_e_ref, out_e_ref)
    with jax.named_scope("sent"):
        sent((STATS, 1), stats_in.at[1])


def pass_kernel(first_ref, second_ref, out_first_ref, out_second_ref):
    out_first_ref[...] = first_ref[...]
    out_second_ref[...] = second_ref[...]


def fused_device(
    outer_gate,
    inner_gate,
    conv_value,
    conv_taps,
    mix_out,
    gain_mixer,
    bias_mixer,
    moe_input,
    route_ids,
    route_weights,
    expert_gate,
    expert_up,
    expert_down,
    shared_gate,
    shared_up,
    shared_down,
    gain_experts,
    bias_experts,
):
    rows, cols = outer_gate.shape
    width = moe_input.shape[1]
    ep_count = lax.axis_size("ep")
    tp_count = lax.axis_size("tp")
    chips = ep_count // CORES
    capacity = max(2, 3 * rows * route_ids.shape[1] // (2 * ep_count))
    seq_length = rows * ep_count // SEQS
    bf16, f32 = jnp.bfloat16, jnp.float32
    vmem = pl.BlockSpec(memory_space=pltpu.VMEM)
    hbm = pl.BlockSpec(memory_space=pl.ANY)
    copies = 5 * chips + 23
    weight = pltpu.VMEM((width, cols), bf16)
    scratch = [
        *([pltpu.VMEM((rows, cols), bf16)] * 3),
        pltpu.VMEM(conv_taps.shape, bf16),
        pltpu.VMEM(route_ids.shape[::-1], jnp.int32),
        pltpu.VMEM(route_weights.shape[::-1], f32),
        *([pltpu.VMEM((cols,), bf16)] * 4),
        *([weight] * 7),
        pltpu.VMEM((chips, CORES, rows, width), bf16),
        pltpu.VMEM((chips, CORES, ep_count, rows), f32),
        pltpu.VMEM((CORES * capacity, width), bf16),
        pltpu.VMEM((chips, CORES * capacity, width), bf16),
        pltpu.VMEM((rows, width), bf16),
        pltpu.VMEM((rows, width), bf16),
        pltpu.VMEM((16, cols), bf16),
        pltpu.VMEM((16, cols), bf16),
        pltpu.VMEM((rows + 16, cols), f32),
        pltpu.VMEM((chips, rows, cols), bf16),
        pltpu.VMEM((chips, rows, cols), bf16),
        pltpu.VMEM((chips, rows, cols), bf16),
        pltpu.VMEM((chips, rows, cols), bf16),
        pltpu.VMEM((2, 8, rows), f32),
        pltpu.VMEM((2, tp_count - 1, 8, rows), f32),
        pltpu.VMEM((rows, cols), f32),
        pltpu.VMEM((rows, cols), f32),
        pltpu.SemaphoreType.DMA((18,)),
        pltpu.SemaphoreType.DMA((chips + 22,)),
        pltpu.SemaphoreType.DMA((copies,)),
        pltpu.SemaphoreType.DMA((chips, tp_count)),
        pltpu.SemaphoreType.DMA((chips,)),
        pltpu.SemaphoreType.DMA((chips,)),
    ]
    out = jax.ShapeDtypeStruct((rows, cols), bf16)
    near = pltpu.VMEM((rows, cols), bf16)
    given = (
        outer_gate,
        inner_gate,
        conv_value,
        conv_taps,
        mix_out,
        gain_mixer,
        bias_mixer,
        moe_input,
        route_ids.T,
        route_weights.T,
        expert_gate,
        expert_up,
        expert_down,
        shared_gate,
        shared_up,
        shared_down,
        gain_experts,
        bias_experts,
    )
    first, second = pl.pallas_call(
        functools.partial(fused_kernel, (ep_count, tp_count, capacity, seq_length)),
        out_shape=(near, near),
        in_specs=[hbm] * 18,
        out_specs=(vmem, vmem),
        scratch_shapes=scratch,
        compiler_params=pltpu.CompilerParams(
            collective_id=0, has_side_effects=True, vmem_limit_bytes=VMEM_BYTES
        ),
    )(*(pltpu.with_memory_space_constraint(one, pltpu.HBM) for one in given))
    return pl.pallas_call(
        pass_kernel,
        out_shape=(out, out),
        in_specs=[vmem, vmem],
        out_specs=(vmem, vmem),
        compiler_params=pltpu.CompilerParams(vmem_limit_bytes=SMALL_BYTES),

    )(first, second)


def on_device(*arrays):
    local_experts = arrays[10].shape[0]
    square = lax.axis_size("tp") == PLANE * PLANE
    if square and local_experts == 1 and lax.axis_size("ep") == CORES * LINE:
        return fused_device(*arrays)
    return plain_device(*arrays)


def solution(mesh):
    in_specs = (
        P("ep", "tp"),
        P("ep", "tp"),
        P("ep", "tp"),
        P(None, "tp"),
        P(None, "tp"),
        P("tp"),
        P("tp"),
        P("ep", None),
        P("ep", None),
        P("ep", None),
        P("ep", None, "tp"),
        P("ep", None, "tp"),
        P("ep", None, "tp"),
        P(None, "tp"),
        P(None, "tp"),
        P(None, "tp"),
        P("tp"),
        P("tp"),
    )
    out_specs = (P("ep", "tp"), P("ep", "tp"))
    return jax.shard_map(
        on_device, mesh=mesh, in_specs=in_specs, out_specs=out_specs, check_vma=False
    )
```

```python
import functools
import types

import jax
import jax.numpy as jnp
from jax import lax
from jax.experimental import pallas as pl
from jax.experimental.pallas import tpu as pltpu
from jax.sharding import PartitionSpec as P

SEQS = 1


def shifted(block, axis, distance):
    devices = range(lax.axis_size(axis))
    route = [(i - distance, i) for i in devices if i - distance in devices]
    return lax.ppermute(block, axis, route)


def finish(values, totals, squares, full_width, gain, offset_bias):
    average = (totals / full_width)[:, None]
    spread = (squares / full_width)[:, None] - average * average
    scaled = (values - average) * lax.rsqrt(spread + 1e-05)
    return (scaled * gain.astype(jnp.float32) + offset_bias.astype(jnp.float32)).astype(
        jnp.bfloat16
    )


def plain_device(
    outer_gate,
    inner_gate,
    conv_value,
    conv_taps,
    mix_out,
    gain_mixer,
    bias_mixer,
    moe_input,
    route_ids,
    route_weights,
    expert_gate,
    expert_up,
    expert_down,
    shared_gate,
    shared_up,
    shared_down,
    gain_experts,
    bias_experts,
):
    token_rows = outer_gate.shape[0]
    column_count = outer_gate.shape[1]
    ep_count = lax.axis_size("ep")
    tp_count = lax.axis_size("tp")
    taps_count = conv_taps.shape[0]
    product = (inner_gate.astype(jnp.float32) * conv_value.astype(jnp.float32)).astype(jnp.bfloat16)
    border = shifted(product[token_rows - (taps_count - 1) :], "ep", 1)
    extended = jnp.concatenate([border, product], axis=0).astype(jnp.float32)
    seq_length = token_rows * ep_count // SEQS
    places = (
        lax.axis_index("ep") * token_rows + jnp.arange(token_rows, dtype=jnp.int32)
    ) % seq_length
    convolved = jnp.zeros((token_rows, column_count), jnp.float32)
    for offset in range(taps_count):
        delay_rows = taps_count - 1 - offset
        delayed = extended[offset : offset + token_rows]
        kept_mask = (places >= delay_rows).astype(jnp.float32)[:, None]
        convolved = convolved + conv_taps[offset].astype(jnp.float32)[None, :] * delayed * kept_mask
    weighted_in = (outer_gate.astype(jnp.float32) * convolved).astype(jnp.bfloat16)
    block = mix_out
    mixed = jnp.dot(
        lax.all_gather(weighted_in, "tp", axis=1, tiled=True),
        block,
        preferred_element_type=jnp.float32,
    )
    topk_count = route_ids.shape[1]
    local_experts = expert_gate.shape[0]
    expert_count = local_experts * ep_count
    capacity = max(2, 3 * token_rows * topk_count // (2 * expert_count))
    flat_ids = route_ids.reshape(-1)
    marks = (flat_ids[:, None] == jnp.arange(expert_count, dtype=jnp.int32)[None, :]).astype(
        jnp.int32
    )
    ranks = jnp.sum((jnp.cumsum(marks, axis=0) - marks) * marks, axis=1)
    targets = flat_ids * capacity + ranks
    sources = jnp.arange(flat_ids.shape[0], dtype=jnp.int32) // topk_count
    sent_rows = lax.dynamic_slice_in_dim(
        moe_input, lax.axis_index("tp") * column_count, column_count, 1
    )
    buffer_rows = jnp.zeros((expert_count * capacity, sent_rows.shape[1]), jnp.bfloat16)
    buffer_rows = buffer_rows.at[targets].set(sent_rows[sources])
    sectioned = buffer_rows.reshape(ep_count, local_experts * capacity, sent_rows.shape[1])
    arrived = lax.all_to_all(sectioned, "ep", split_axis=0, concat_axis=0, tiled=True)
    arrived = lax.all_gather(arrived, "tp", axis=2, tiled=True)
    expert_rows = arrived.reshape(ep_count, local_experts, capacity, arrived.shape[2])
    gate_value = jnp.einsum(
        "secd,edf->secf", expert_rows, expert_gate, preferred_element_type=jnp.float32
    )
    up_value = jnp.einsum(
        "secd,edf->secf", expert_rows, expert_up, preferred_element_type=jnp.float32
    )
    hidden = (jax.nn.silu(gate_value) * up_value).astype(jnp.bfloat16)
    flat_hidden = hidden.reshape(expert_count * capacity, hidden.shape[3])
    shared_gate_value = jnp.dot(moe_input, shared_gate, preferred_element_type=jnp.float32)
    shared_up_value = jnp.dot(moe_input, shared_up, preferred_element_type=jnp.float32)
    shared_hidden = (jax.nn.silu(shared_gate_value) * shared_up_value).astype(jnp.bfloat16)
    piece = lax.all_gather(flat_hidden, "tp", axis=1, tiled=True)
    block = expert_down
    shaped = piece.reshape(ep_count, local_experts, capacity, piece.shape[1])
    routed_sum = jnp.einsum("secf,efd->secd", shaped, block, preferred_element_type=jnp.float32)
    block = shared_down
    shared_sum = jnp.dot(
        lax.all_gather(shared_hidden, "tp", axis=1, tiled=True),
        block,
        preferred_element_type=jnp.float32,
    )
    expert_out = routed_sum.astype(jnp.bfloat16).reshape(
        ep_count, local_experts * capacity, column_count
    )
    returned = lax.all_to_all(expert_out, "ep", split_axis=0, concat_axis=0, tiled=True)
    picked = returned.reshape(expert_count * capacity, column_count)[targets].astype(jnp.float32)
    weighted = picked.reshape(token_rows, topk_count, column_count) * route_weights[:, :, None]
    combined = jnp.sum(weighted, axis=1) + shared_sum
    mixer_total, mixer_square, expert_total, expert_square = lax.psum(
        (
            jnp.sum(mixed, axis=1),
            jnp.sum(mixed * mixed, axis=1),
            jnp.sum(combined, axis=1),
            jnp.sum(combined * combined, axis=1),
        ),
        "tp",
    )
    full_width = column_count * tp_count
    out_mixer = finish(mixed, mixer_total, mixer_square, full_width, gain_mixer, bias_mixer)
    out_experts = finish(
        combined, expert_total, expert_square, full_width, gain_experts, bias_experts
    )
    return (out_mixer, out_experts)


PLANE = 2
SMALL_BYTES = 4 * 1024 * 1024
CORES = 2
VMEM_BYTES = 48 * 1024 * 1024


(
    UP,
    DOWN,
    ROUTE,
    PAIR,
    EDGE,
    CROSS,
    HIDDEN,
    SHARED,
    MIXER,
    PART,
    RETURN,
    STATS,
    ONWARD,
    ROUTE_UP,
    ROUTE_DOWN,
) = range(15)
LINE = 4
ALL, INNER, OUTER = range(3)


def plan(act):
    return [
        (ALL, act.shared, ()),
        (ALL, act.up, (0,)),
        (ALL, act.start_y, (0,)),
        (ALL, act.start_x, (0, 0)),
        (ALL, act.line, (1, 0, True)),
        (INNER, act.line, (2, 0)),
        (ALL, act.start_x, (0, 1)),
        (ALL, act.line, (1, 1, True)),
        (INNER, act.line, (2, 1)),
        (ALL, act.shared_relay, ()),
        (OUTER, act.line, (2, 0, True)),
        (INNER, act.line, (2, 2)),
        (INNER, act.line, (3, 0)),
        (ALL, act.cross, (1, 2)),
        (ALL, act.cross, (1, 3)),
        (INNER, act.line, (2, 3)),
        (OUTER, act.line, (2, 1, True)),
        (INNER, act.line, (3, 1)),
        (ALL, act.up, (1,)),
        (ALL, act.start, (1,)),
        (INNER, act.line, (3, 2)),
        (OUTER, act.line, (3, 0)),
        (OUTER, act.cross, (2, 2)),
        (OUTER, act.cross, (2, 3)),
        (OUTER, act.line, (3, 1)),
        (OUTER, act.relay, (0,)),
        (ALL, act.up, (2,)),
        (ALL, act.start, (2,)),
        (INNER, act.line, (3, 3)),
        (ALL, act.shared_dot, ()),
        (OUTER, act.line, (3, 2)),
        (OUTER, act.line, (3, 3)),
        (INNER, act.relay, (1,)),
        (ALL, act.up_part, (3, 0)),
        (ALL, act.start_part, (3, 0)),
        (INNER, act.relay, (2,)),
        (ALL, act.up_part, (3, 1)),
        (ALL, act.start_part, (3, 1)),
        (INNER, act.down, (1,)),
        (INNER, act.give_back, (1,)),
        (ALL, act.relay_part, (3, 0)),
        (INNER, act.down, (2,)),
        (ALL, act.relay_part, (3, 1)),
        (INNER, act.give_back, (2,)),
        (OUTER, act.relay, (2,)),
        (OUTER, act.relay, (1,)),
        (ALL, act.mixer, ()),
        (INNER, act.relay, (0,)),
        (ALL, act.down_part, (3, 0)),
        (ALL, act.give_back_part, (3, 0)),
        (ALL, act.down_part, (3, 1)),
        (ALL, act.give_back_part, (3, 1)),
        (OUTER, act.down, (2,)),
        (OUTER, act.down, (1,)),
        (OUTER, act.give_back, (2,)),
        (ALL, act.mixer_relay, (0,)),
        (OUTER, act.give_back, (1,)),
        (ALL, act.mixer_relay, (1,)),
        (ALL, act.down, (0,)),
        (ALL, act.give_back, (0,)),
        (ALL, act.mixer_dot, ()),
        (ALL, act.collect, (1,)),
        (ALL, act.collect, (2,)),
        (ALL, act.collect, (3,)),
    ]


def nearest_first(chips):
    def key(z):
        return lambda k: (abs(k - z), abs(2 * k - (chips - 1)))

    return [sorted((k for k in range(chips) if k != z), key=key(z)) for z in range(chips)]


def silu(value):
    return value / (1.0 + jnp.exp(-value))


def fused_kernel(
    shape,
    outer_hbm,
    inner_hbm,
    value_hbm,
    taps_hbm,
    mix_hbm,
    gain_m_hbm,
    bias_m_hbm,
    moe_hbm,
    ids_hbm,
    route_w_hbm,
    gate_hbm,
    up_hbm,
    down_hbm,
    shared_gate_hbm,
    shared_up_hbm,
    shared_down_hbm,
    gain_e_hbm,
    bias_e_hbm,
    out_m_ref,
    out_e_ref,
    outer_ref,
    inner_ref,
    value_ref,
    taps_ref,
    ids_ref,
    route_w_ref,
    gain_m_ref,
    bias_m_ref,
    gain_e_ref,
    bias_e_ref,
    mix_v,
    gate_v,
    up_v,
    down_v,
    shared_gate_v,
    shared_up_v,
    shared_down_v,
    tokens,
    route,
    rows_in,
    hidden,
    weighted,
    shared_hidden,
    border,
    edge,
    extended,
    peer_part,
    own_part,
    sent_sum,
    returned,
    stats_out,
    stats_in,
    mixed_ref,
    total_ref,
    load_sem,
    send_sem,
    recv_sem,
    line_recv,
    route_recv,
    return_recv,
):
    ep_count, tp_count, capacity, seq_length = shape
    chips = ep_count // CORES
    rows, cols = outer_ref.shape
    full_width = cols * tp_count
    me = lax.axis_index("ep")
    j = lax.axis_index("tp")
    z = me // CORES
    c = me % CORES
    x = j % PLANE
    y = j // PLANE
    jx = y * PLANE + (1 - x)
    jy = (1 - y) * PLANE + x
    jd = (1 - y) * PLANE + (1 - x)
    other = z * CORES + (1 - c)
    f32, bf16 = jnp.float32, jnp.bfloat16

    orders = nearest_first(chips)

    def pick(values):
        chosen = jnp.int32(values[0])
        for k in range(1, chips):
            chosen = jnp.where(z == k, values[k], chosen)
        return chosen

    sources = [z] + [pick([orders[k][s - 1] for k in range(chips)]) for s in range(1, chips)]

    def whole(k, q):
        s = orders[k].index(q) + 1
        return s == chips - 1 or s == chips - 2 and 0 < k < chips - 1

    def onward_of(k, s):
        q = orders[k][s - 1]
        n = k + 1 if q < k else k - 1
        there = 0 <= n < chips
        return n if there else k, there, there and whole(n, q)

    rising = pick([int(k + 1 < chips and whole(k + 1, k)) for k in range(chips)]) > 0
    falling = pick([int(k > 0 and whole(k - 1, k)) for k in range(chips)]) > 0

    loads = []

    def load(source, target):
        loads.append(pltpu.make_async_copy(source, target, load_sem.at[len(loads)]))
        loads[-1].start()
        return loads[-1]

    above = (z + 1) % chips
    below = (z + chips - 1) % chips
    higher = z + 1 < chips
    lower = z > 0
    beside = jnp.where(c > 0, me + 1, me + ep_count - 1) % ep_count
    slanted = jnp.where(c > 0, z + 1 < chips, z > 0)

    barrier = pltpu.get_barrier_semaphore()

    def greet(row, column):
        pl.semaphore_signal(
            barrier, inc=1, device_id=(row, column), device_id_type=pl.DeviceIdType.MESH
        )

    greet(other, j)
    greet(me, jx)
    greet(me, jy)
    pl.when(higher)(lambda: greet(above * CORES + c, j))
    pl.when(lower)(lambda: greet(below * CORES + c, j))
    pl.when(slanted)(lambda: greet(beside, j))
    greeted = 3 + higher.astype(jnp.int32) + lower.astype(jnp.int32) + slanted.astype(jnp.int32)

    moe_load = load(moe_hbm, tokens.at[z, 0])
    ids_load = load(ids_hbm, ids_ref)
    route_w_load = load(route_w_hbm, route_w_ref)
    inner_load = load(inner_hbm, inner_ref)
    value_load = load(value_hbm, value_ref)
    shared_gate_load = load(shared_gate_hbm, shared_gate_v)
    shared_up_load = load(shared_up_hbm, shared_up_v)
    gate_load = load(gate_hbm.at[0], gate_v)
    up_load = load(up_hbm.at[0], up_v)
    outer_load = load(outer_hbm, outer_ref)
    taps_load = load(taps_hbm, taps_ref)
    gain_m_load = load(gain_m_hbm, gain_m_ref)
    bias_m_load = load(bias_m_hbm, bias_m_ref)
    gain_e_load = load(gain_e_hbm, gain_e_ref)
    bias_e_load = load(bias_e_hbm, bias_e_ref)
    shared_down_load = load(shared_down_hbm, shared_down_v)
    down_load = load(down_hbm.at[0], down_v)
    mix_load = load(mix_hbm, mix_v)

    def loaded(*several):
        for one in several:
            one.wait()

    loaded(moe_load)
    with jax.named_scope("barrier"):
        pl.semaphore_wait(barrier, greeted)

    groups = {}
    numbers = {}

    def remote(source, target, sent, received, device):
        return pltpu.make_async_remote_copy(
            src_ref=source,
            dst_ref=target,
            send_sem=sent,
            recv_sem=received,
            device_id=device,
            device_id_type=pl.DeviceIdType.MESH,
        )

    def group(name):
        return send_sem.at[groups.setdefault(name, len(groups))]

    def number(name):
        return recv_sem.at[numbers.setdefault(name, len(numbers))]

    def send(many, name, source, target, device, received=None, when=None):
        copy = remote(source, target, group(many), number(name) if received is None else received, device)
        if when is None:
            copy.start()
        else:
            pl.when(when)(copy.start)

    def arrive(name, target, received=None):
        remote(target, target, group(EDGE), number(name) if received is None else received, (other, j)).wait_recv()

    def sent(many, ref, when=None):
        def wait():
            remote(ref, ref, group(many), number(EDGE), (other, j)).wait_send()

        if when is None:
            wait()
        else:
            pl.when(when)(wait)

    def columns(owner):
        return pl.ds(pl.multiple_of(owner * cols, cols), cols)

    def gather_x(name, ref):
        part = ref.at[:, columns(j)]
        send(name[0], name + (0,), part, part, (me, jx))

    def gather_y(name, ref):
        part = ref.at[:, columns(j)]
        send(name[0], name + (1,), part, part, (me, jy))

    def relay_x(name, ref):
        half = ref.shape[0] // 2
        arrive(name + (0,), ref.at[:, columns(jx)])
        part = ref.at[pl.ds(0, half), columns(jx)]
        send(name[0], name + (2,), part, part, (me, jy))

    def relay_y(name, ref):
        half = ref.shape[0] // 2
        arrive(name + (1,), ref.at[:, columns(jy)])
        part = ref.at[pl.ds(half, half), columns(jy)]
        send(name[0], name + (2,), part, part, (me, jx))

    def gather_finish(name, ref):
        arrive(name + (2,), ref.at[:, columns(jd)])

    quarters = (x, PLANE + y, 1 - x, PLANE + 1 - y)
    def line_start(k):
        part = tokens.at[z, 0, :, columns(quarters[k])]
        received = line_recv.at[z, k]
        more = k - k % PLANE
        device = (above * CORES + c, j)
        send((UP, more), (), part, part, device, received, rising if more else higher)
        device = (below * CORES + c, j)
        send((DOWN, more), (), part, part, device, received, falling if more else lower)

    line_start(0)
    send(PAIR, (PAIR, 0), tokens.at[z, 0], tokens.at[z, 1], (other, j))
    loaded(ids_load, route_w_load)
    named = lax.broadcasted_iota(jnp.int32, (ep_count, rows), 0)
    dense = jnp.zeros((ep_count, rows), f32)
    for k in range(ids_ref.shape[0]):
        dense = dense + jnp.where(named == ids_ref[k : k + 1, :], route_w_ref[k : k + 1, :], 0.0)
    route[z, 0] = dense
    own = route.at[z, 0]
    send(ROUTE_UP, (), own, own, (above * CORES + c, j), route_recv.at[z], higher)
    send(ROUTE_DOWN, (), own, own, (below * CORES + c, j), route_recv.at[z], lower)
    send(ROUTE, (ROUTE, 0), own, route.at[z, 1], (other, j))
    line_start(1)
    line_start(2)
    line_start(3)
    loaded(inner_load, value_load)
    product = (inner_ref[...].astype(f32) * value_ref[...].astype(f32)).astype(bf16)
    edge_rows = edge.shape[0]
    edge[...] = product[rows - edge_rows :]

    @pl.when(me == 0)
    def _():
        border[...] = jnp.zeros_like(border)

    pad = extended.shape[0] - rows
    extended[pad:, :] = product.astype(f32)
    last = me == ep_count - 1
    send(EDGE, EDGE, edge, border, ((me + 1) % ep_count, j), None, ~last)

    def dot(a, b):
        return jnp.dot(a, b, preferred_element_type=f32)

    def choice(s, p):
        weight = route[sources[s], p, pl.ds(me, 1), :]
        routed = (weight > 0.0).astype(f32)
        earlier = lax.broadcasted_iota(jnp.int32, (rows, rows), 0)
        later = lax.broadcasted_iota(jnp.int32, (rows, rows), 1)
        upper = (earlier <= later).astype(f32).astype(bf16)
        many = jnp.broadcast_to(routed, (16, rows)).astype(bf16)
        rank = dot(many, upper)[0:1, :] * routed
        slot = lax.broadcasted_iota(jnp.int32, (capacity, rows), 0).astype(f32) + 1.0
        return (slot == rank).astype(f32), weight

    def line_arrival(s, k, swap=False):
        q = sources[s]
        quarter = quarters[k]
        part = tokens.at[q, 0, :, columns(quarter)]
        if k == 1:
            own = route.at[q, 0]
            arrive((), own, route_recv.at[q])
            if (s, k) in onwards:
                onward, more = onwards[s, k]
                device = (onward * CORES + c, j)
                send((ROUTE, s), (), own, own, device, route_recv.at[q], more)
            send(ROUTE, (ROUTE, s), own, route.at[q, 1], (other, j))
        arrive((), part, line_recv.at[q, k])
        onward_send(s, k)
        if swap:
            send((CROSS, s), (CROSS, s, k), part, part, (me, (jx, jy)[k]))
        send(PAIR, (PAIR, s), part, tokens.at[q, 1, :, columns(quarter)], (other, j))

    onwards = {}
    for s in range(1, chips):
        for k in range(tp_count):
            told = [onward_of(n, s)[1 if k < PLANE else 2] for n in range(chips)]
            if any(told):
                onward = pick([onward_of(n, s)[0] for n in range(chips)])
                onwards[s, k] = (onward, pick([int(t) for t in told]) > 0)

    def onward_send(s, k):
        q = sources[s]
        part = tokens.at[q, 0, :, columns(quarters[k])]
        if (s, k) in onwards:
            onward, more = onwards[s, k]
            device = (onward * CORES + c, j)
            send((ONWARD, s, k - k % PLANE), (), part, part, device, line_recv.at[q, k], more)

    def cross_arrival(s, k):
        q = sources[s]
        part = tokens.at[q, 0, :, columns(quarters[k])]
        arrive((CROSS, s, k - PLANE), part)
        onward_send(s, k)
        send(PAIR, (PAIR, s), part, tokens.at[q, 1, :, columns(quarters[k])], (other, j))

    def expert_up(s):
        q = sources[s]
        arrive((ROUTE, s), route.at[q, 1])
        if s == 0:
            loaded(gate_load, up_load)
        for p in range(CORES):
            picks, _ = choice(s, p)
            if p == 1:
                arrive((PAIR, s), tokens.at[q, 1])
            rows_in[p * capacity : (p + 1) * capacity, :] = dot(
                picks.astype(bf16), tokens[q, p]
            ).astype(bf16)
        held = silu(dot(rows_in[...], gate_v[...])) * dot(rows_in[...], up_v[...])
        hidden[q, :, columns(j)] = held.astype(bf16)

    def up_part(s, t):
        q = sources[s]
        p = (t + c) % CORES
        if t == 0:
            arrive((ROUTE, s), route.at[q, 1])
            arrive((PAIR, s), tokens.at[q, 1])
        picks, _ = choice(s, p)
        taken = dot(picks.astype(bf16), tokens[q, p]).astype(bf16)
        held = silu(dot(taken, gate_v[...])) * dot(taken, up_v[...])
        hidden[q, t * capacity : (t + 1) * capacity, columns(j)] = held.astype(bf16)

    def part_ref(s, t):
        return hidden.at[sources[s], pl.ds(t * capacity, capacity)]

    def down_part(s, t):
        q = sources[s]
        gather_finish((HIDDEN, s, t), part_ref(s, t))
        picks, weight = choice(s, (t + c) % CORES)
        full = dot(hidden[q, t * capacity : (t + 1) * capacity], down_v[...])
        scale = jnp.sum(picks * weight, axis=1, keepdims=True)
        scaled = (full * scale).astype(bf16)
        spread = lax.dot_general(
            picks.astype(bf16), scaled, (((0,), (0,)), ((), ())), preferred_element_type=f32
        ).astype(bf16)

        @pl.when(c == t)
        def _():
            sent_sum[q] = spread

        @pl.when(c != t)
        def _():
            own_part[q] = spread
            send(PART, (PART, s), own_part.at[q], peer_part.at[q], (other, j))

    def return_part(s, t):
        @pl.when(c == t)
        def _():
            expert_return(s)

    def start_x(s, t=None):
        ref = hidden.at[sources[s]] if t is None else part_ref(s, t)
        gather_x((HIDDEN, s), ref)

    def start_y(s):
        gather_y((HIDDEN, s), hidden.at[sources[s]])

    def start(s):
        start_x(s)
        start_y(s)

    def relay(s):
        relay_x((HIDDEN, s), hidden.at[sources[s]])
        relay_y((HIDDEN, s), hidden.at[sources[s]])

    def start_part(s, t):
        gather_x((HIDDEN, s, t), part_ref(s, t))
        gather_y((HIDDEN, s, t), part_ref(s, t))

    def relay_part(s, t):
        relay_x((HIDDEN, s, t), part_ref(s, t))
        relay_y((HIDDEN, s, t), part_ref(s, t))

    def collect(s):
        q = sources[s]
        arrive((), returned.at[q], return_recv.at[q])
        total_ref[...] = total_ref[...] + returned[q].astype(f32)

    def expert_down(s):
        q = sources[s]
        gather_finish((HIDDEN, s), hidden.at[q])
        full = dot(hidden[q], down_v[...])
        for p in reversed(range(CORES)):
            picks, weight = choice(s, p)
            scale = jnp.sum(picks * weight, axis=1, keepdims=True)
            scaled = (full[p * capacity : (p + 1) * capacity] * scale).astype(bf16)
            spread = lax.dot_general(
                picks.astype(bf16), scaled, (((0,), (0,)), ((), ())), preferred_element_type=f32
            )
            if p == 1:
                own_part[q] = spread.astype(bf16)
                send(PART, (PART, s), own_part.at[q], peer_part.at[q], (other, j))
            elif s == 0:
                total_ref[...] = total_ref[...] + spread
            else:
                sent_sum[q] = spread.astype(bf16)

    def expert_return(s):
        q = sources[s]
        arrive((PART, s), peer_part.at[q])
        if s == 0:
            total_ref[...] = total_ref[...] + peer_part[q].astype(f32)
        else:
            sent_sum[q] = (sent_sum[q].astype(f32) + peer_part[q].astype(f32)).astype(bf16)
            send(RETURN, (), sent_sum.at[q], returned.at[z], (q * CORES + c, j), return_recv.at[z])

    def stats_start(k, values):
        lane = lax.broadcasted_iota(jnp.int32, (rows, rows), 1)
        total = jnp.sum(values, axis=1, keepdims=True)
        square = jnp.sum(values * values, axis=1, keepdims=True)
        tile = jnp.where(lane == 0, total, jnp.where(lane == 1, square, 0.0))
        stats_out[k] = tile.T[0 : stats_out.shape[1], :]
        for n, peer in enumerate((jx, jy, jd)):
            send((STATS, k), (STATS, k), stats_out.at[k], stats_in.at[k, n], (me, peer))

    def stats_finish(k, values, gain_ref, bias_ref, out_ref):
        tile = stats_out[k]
        arrive((STATS, k), stats_in.at[k])
        for n in range(tp_count - 1):
            tile = tile + stats_in[k, n]
        padded = jnp.concatenate(
            [tile, jnp.zeros((rows - tile.shape[0], rows), f32)], axis=0
        ).T
        average = padded[:, 0:1] / full_width
        spread = padded[:, 1:2] / full_width - average * average
        scaled = (values - average) * lax.rsqrt(spread + 1e-05)
        out_ref[...] = (
            scaled * gain_ref[...].astype(f32).reshape(1, cols)
            + bias_ref[...].astype(f32).reshape(1, cols)
        ).astype(bf16)

    def shared_start():
        loaded(shared_gate_load, shared_up_load)
        own = tokens[z, 0]
        held = silu(dot(own, shared_gate_v[...])) * dot(own, shared_up_v[...])
        shared_hidden[:, columns(j)] = held.astype(bf16)
        gather_x((SHARED,), shared_hidden)
        gather_y((SHARED,), shared_hidden)

    def mixer_ref(t):
        return weighted.at[pl.ds(t * (rows // 2), rows // 2)]

    def mixer_start():
        pl.when(me > 0)(lambda: arrive(EDGE, border))
        loaded(outer_load, taps_load)
        extended[pad - edge_rows : pad, :] = border[...].astype(f32)
        places = (me * rows + lax.broadcasted_iota(jnp.int32, (rows, 1), 0)) % seq_length
        taps_count = taps_ref.shape[0]
        convolved = jnp.zeros((rows, cols), f32)
        for offset in range(taps_count):
            delay = taps_count - 1 - offset
            delayed = extended[pad - delay : pad - delay + rows, :]
            kept = (places >= delay).astype(f32)
            convolved = convolved + taps_ref[offset : offset + 1, :].astype(f32) * delayed * kept
        weighted[:, columns(j)] = (outer_ref[...].astype(f32) * convolved).astype(bf16)
        for t in range(2):
            gather_x((MIXER, t), mixer_ref(t))
            gather_y((MIXER, t), mixer_ref(t))

    def shared_relay():
        relay_x((SHARED,), shared_hidden)
        relay_y((SHARED,), shared_hidden)

    def mixer_relay(t):
        relay_x((MIXER, t), mixer_ref(t))
        relay_y((MIXER, t), mixer_ref(t))

    def mixer_dot():
        gather_finish((MIXER, 0), mixer_ref(0))
        gather_finish((MIXER, 1), mixer_ref(1))
        loaded(mix_load)
        mixed_ref[...] = dot(weighted[...], mix_v[...])
        stats_start(0, mixed_ref[...])

    def mixer_end():
        loaded(gain_m_load, bias_m_load, gain_e_load, bias_e_load)
        stats_finish(0, mixed_ref[...], gain_m_ref, bias_m_ref, out_m_ref)

    def shared_dot():
        gather_finish((SHARED,), shared_hidden)
        loaded(shared_down_load, down_load)
        total_ref[...] = dot(shared_hidden[...], shared_down_v[...])

    act = types.SimpleNamespace(
        shared=shared_start,
        up=expert_up,
        start=start,
        start_x=start_x,
        start_y=start_y,
        line=line_arrival,
        cross=cross_arrival,
        relay=relay,
        down=expert_down,
        give_back=expert_return,
        up_part=up_part,
        start_part=start_part,
        relay_part=relay_part,
        down_part=down_part,
        give_back_part=return_part,
        shared_relay=shared_relay,
        shared_dot=shared_dot,
        mixer=mixer_start,
        mixer_relay=mixer_relay,
        mixer_dot=mixer_dot,
        collect=collect,
    )
    inner = (z > 0) & (z < chips - 1)
    for where, step, which in plan(act):
        if where == ALL:
            step(*which)
        else:
            pl.when(inner if where == INNER else ~inner)(functools.partial(step, *which))
    with jax.named_scope("stats"):
        stats_start(1, total_ref[...])
    with jax.named_scope("mixer_end"):
        mixer_end()
    with jax.named_scope("drain"):
        lines = tokens.at[0, 0, :, pl.ds(0, PLANE * cols)]
        sent((UP, 0), lines, higher)
        sent((DOWN, 0), lines, lower)
        sent((UP, PLANE), lines, rising)
        sent((DOWN, PLANE), lines, falling)
        for s, k in onwards:
            if k % PLANE == 0:
                sent((ONWARD, s, k), lines, onwards[s, k][1])
            if k == 0:
                sent((ROUTE, s), route.at[0, 0], onwards[s, k][1])
        sent(ROUTE_UP, route.at[0, 0], higher)
        sent(ROUTE_DOWN, route.at[0, 0], lower)
        sent(PAIR, tokens.at[:, 0])
        sent(ROUTE, route.at[:, 0])
        sent(EDGE, edge, ~last)
        sent((CROSS, 1), lines)
        sent((CROSS, 2), lines, ~inner)
        gathered = pl.ds(0, (tp_count - 1) * cols)
        sent(HIDDEN, hidden.at[:, :, gathered])
        sent(SHARED, shared_hidden.at[:, gathered])
        sent(MIXER, weighted.at[:, gathered])
        sent(PART, own_part)
        sent(RETURN, own_part.at[pl.ds(0, chips - 1)])
        sent((STATS, 0), stats_in.at[0])
    with jax.named_scope("finish"):
        stats_finish(1, total_ref[...], gain_e_ref, bias_e_ref, out_e_ref)
    with jax.named_scope("sent"):
        sent((STATS, 1), stats_in.at[1])


def pass_kernel(first_ref, second_ref, out_first_ref, out_second_ref):
    out_first_ref[...] = first_ref[...]
    out_second_ref[...] = second_ref[...]


def fused_device(
    outer_gate,
    inner_gate,
    conv_value,
    conv_taps,
    mix_out,
    gain_mixer,
    bias_mixer,
    moe_input,
    route_ids,
    route_weights,
    expert_gate,
    expert_up,
    expert_down,
    shared_gate,
    shared_up,
    shared_down,
    gain_experts,
    bias_experts,
):
    rows, cols = outer_gate.shape
    width = moe_input.shape[1]
    ep_count = lax.axis_size("ep")
    tp_count = lax.axis_size("tp")
    chips = ep_count // CORES
    capacity = max(2, 3 * rows * route_ids.shape[1] // (2 * ep_count))
    seq_length = rows * ep_count // SEQS
    bf16, f32 = jnp.bfloat16, jnp.float32
    vmem = pl.BlockSpec(memory_space=pltpu.VMEM)
    hbm = pl.BlockSpec(memory_space=pl.ANY)
    copies = 5 * chips + 23
    weight = pltpu.VMEM((width, cols), bf16)
    scratch = [
        *([pltpu.VMEM((rows, cols), bf16)] * 3),
        pltpu.VMEM(conv_taps.shape, bf16),
        pltpu.VMEM(route_ids.shape[::-1], jnp.int32),
        pltpu.VMEM(route_weights.shape[::-1], f32),
        *([pltpu.VMEM((cols,), bf16)] * 4),
        *([weight] * 7),
        pltpu.VMEM((chips, CORES, rows, width), bf16),
        pltpu.VMEM((chips, CORES, ep_count, rows), f32),
        pltpu.VMEM((CORES * capacity, width), bf16),
        pltpu.VMEM((chips, CORES * capacity, width), bf16),
        pltpu.VMEM((rows, width), bf16),
        pltpu.VMEM((rows, width), bf16),
        pltpu.VMEM((16, cols), bf16),
        pltpu.VMEM((16, cols), bf16),
        pltpu.VMEM((rows + 16, cols), f32),
        pltpu.VMEM((chips, rows, cols), bf16),
        pltpu.VMEM((chips, rows, cols), bf16),
        pltpu.VMEM((chips, rows, cols), bf16),
        pltpu.VMEM((chips, rows, cols), bf16),
        pltpu.VMEM((2, 8, rows), f32),
        pltpu.VMEM((2, tp_count - 1, 8, rows), f32),
        pltpu.VMEM((rows, cols), f32),
        pltpu.VMEM((rows, cols), f32),
        pltpu.SemaphoreType.DMA((18,)),
        pltpu.SemaphoreType.DMA((chips + 22,)),
        pltpu.SemaphoreType.DMA((copies,)),
        pltpu.SemaphoreType.DMA((chips, tp_count)),
        pltpu.SemaphoreType.DMA((chips,)),
        pltpu.SemaphoreType.DMA((chips,)),
    ]
    out = jax.ShapeDtypeStruct((rows, cols), bf16)
    near = pltpu.VMEM((rows, cols), bf16)
    given = (
        outer_gate,
        inner_gate,
        conv_value,
        conv_taps,
        mix_out,
        gain_mixer,
        bias_mixer,
        moe_input,
        route_ids.T,
        route_weights.T,
        expert_gate,
        expert_up,
        expert_down,
        shared_gate,
        shared_up,
        shared_down,
        gain_experts,
        bias_experts,
    )
    first, second = pl.pallas_call(
        functools.partial(fused_kernel, (ep_count, tp_count, capacity, seq_length)),
        out_shape=(near, near),
        in_specs=[hbm] * 18,
        out_specs=(vmem, vmem),
        scratch_shapes=scratch,
        compiler_params=pltpu.CompilerParams(
            collective_id=0, has_side_effects=True, vmem_limit_bytes=VMEM_BYTES
        ),
    )(*(pltpu.with_memory_space_constraint(one, pltpu.HBM) for one in given))
    return pl.pallas_call(
        pass_kernel,
        out_shape=(out, out),
        in_specs=[vmem, vmem],
        out_specs=(vmem, vmem),
        compiler_params=pltpu.CompilerParams(vmem_limit_bytes=SMALL_BYTES),

    )(first, second)


def on_device(*arrays):
    local_experts = arrays[10].shape[0]
    square = lax.axis_size("tp") == PLANE * PLANE
    if square and local_experts == 1 and lax.axis_size("ep") == CORES * LINE:
        return fused_device(*arrays)
    return plain_device(*arrays)


def solution(mesh):
    in_specs = (
        P("ep", "tp"),
        P("ep", "tp"),
        P("ep", "tp"),
        P(None, "tp"),
        P(None, "tp"),
        P("tp"),
        P("tp"),
        P("ep", None),
        P("ep", None),
        P("ep", None),
        P("ep", None, "tp"),
        P("ep", None, "tp"),
        P("ep", None, "tp"),
        P(None, "tp"),
        P(None, "tp"),
        P(None, "tp"),
        P("tp"),
        P("tp"),
    )
    out_specs = (P("ep", "tp"), P("ep", "tp"))
    return jax.shard_map(
        on_device, mesh=mesh, in_specs=in_specs, out_specs=out_specs, check_vma=False
    )
```

```python
import functools
import types

import jax
import jax.numpy as jnp
from jax import lax
from jax.experimental import pallas as pl
from jax.experimental.pallas import tpu as pltpu
from jax.sharding import PartitionSpec as P

SEQS = 1


def shifted(block, axis, distance):
    devices = range(lax.axis_size(axis))
    route = [(i - distance, i) for i in devices if i - distance in devices]
    return lax.ppermute(block, axis, route)


def finish(values, totals, squares, full_width, gain, offset_bias):
    average = (totals / full_width)[:, None]
    spread = (squares / full_width)[:, None] - average * average
    scaled = (values - average) * lax.rsqrt(spread + 1e-05)
    return (scaled * gain.astype(jnp.float32) + offset_bias.astype(jnp.float32)).astype(
        jnp.bfloat16
    )


def plain_device(
    outer_gate,
    inner_gate,
    conv_value,
    conv_taps,
    mix_out,
    gain_mixer,
    bias_mixer,
    moe_input,
    route_ids,
    route_weights,
    expert_gate,
    expert_up,
    expert_down,
    shared_gate,
    shared_up,
    shared_down,
    gain_experts,
    bias_experts,
):
    token_rows = outer_gate.shape[0]
    column_count = outer_gate.shape[1]
    ep_count = lax.axis_size("ep")
    tp_count = lax.axis_size("tp")
    taps_count = conv_taps.shape[0]
    product = (inner_gate.astype(jnp.float32) * conv_value.astype(jnp.float32)).astype(jnp.bfloat16)
    border = shifted(product[token_rows - (taps_count - 1) :], "ep", 1)
    extended = jnp.concatenate([border, product], axis=0).astype(jnp.float32)
    seq_length = token_rows * ep_count // SEQS
    places = (
        lax.axis_index("ep") * token_rows + jnp.arange(token_rows, dtype=jnp.int32)
    ) % seq_length
    convolved = jnp.zeros((token_rows, column_count), jnp.float32)
    for offset in range(taps_count):
        delay_rows = taps_count - 1 - offset
        delayed = extended[offset : offset + token_rows]
        kept_mask = (places >= delay_rows).astype(jnp.float32)[:, None]
        convolved = convolved + conv_taps[offset].astype(jnp.float32)[None, :] * delayed * kept_mask
    weighted_in = (outer_gate.astype(jnp.float32) * convolved).astype(jnp.bfloat16)
    block = mix_out
    mixed = jnp.dot(
        lax.all_gather(weighted_in, "tp", axis=1, tiled=True),
        block,
        preferred_element_type=jnp.float32,
    )
    topk_count = route_ids.shape[1]
    local_experts = expert_gate.shape[0]
    expert_count = local_experts * ep_count
    capacity = max(2, 3 * token_rows * topk_count // (2 * expert_count))
    flat_ids = route_ids.reshape(-1)
    marks = (flat_ids[:, None] == jnp.arange(expert_count, dtype=jnp.int32)[None, :]).astype(
        jnp.int32
    )
    ranks = jnp.sum((jnp.cumsum(marks, axis=0) - marks) * marks, axis=1)
    targets = flat_ids * capacity + ranks
    sources = jnp.arange(flat_ids.shape[0], dtype=jnp.int32) // topk_count
    sent_rows = lax.dynamic_slice_in_dim(
        moe_input, lax.axis_index("tp") * column_count, column_count, 1
    )
    buffer_rows = jnp.zeros((expert_count * capacity, sent_rows.shape[1]), jnp.bfloat16)
    buffer_rows = buffer_rows.at[targets].set(sent_rows[sources])
    sectioned = buffer_rows.reshape(ep_count, local_experts * capacity, sent_rows.shape[1])
    arrived = lax.all_to_all(sectioned, "ep", split_axis=0, concat_axis=0, tiled=True)
    arrived = lax.all_gather(arrived, "tp", axis=2, tiled=True)
    expert_rows = arrived.reshape(ep_count, local_experts, capacity, arrived.shape[2])
    gate_value = jnp.einsum(
        "secd,edf->secf", expert_rows, expert_gate, preferred_element_type=jnp.float32
    )
    up_value = jnp.einsum(
        "secd,edf->secf", expert_rows, expert_up, preferred_element_type=jnp.float32
    )
    hidden = (jax.nn.silu(gate_value) * up_value).astype(jnp.bfloat16)
    flat_hidden = hidden.reshape(expert_count * capacity, hidden.shape[3])
    shared_gate_value = jnp.dot(moe_input, shared_gate, preferred_element_type=jnp.float32)
    shared_up_value = jnp.dot(moe_input, shared_up, preferred_element_type=jnp.float32)
    shared_hidden = (jax.nn.silu(shared_gate_value) * shared_up_value).astype(jnp.bfloat16)
    piece = lax.all_gather(flat_hidden, "tp", axis=1, tiled=True)
    block = expert_down
    shaped = piece.reshape(ep_count, local_experts, capacity, piece.shape[1])
    routed_sum = jnp.einsum("secf,efd->secd", shaped, block, preferred_element_type=jnp.float32)
    block = shared_down
    shared_sum = jnp.dot(
        lax.all_gather(shared_hidden, "tp", axis=1, tiled=True),
        block,
        preferred_element_type=jnp.float32,
    )
    expert_out = routed_sum.astype(jnp.bfloat16).reshape(
        ep_count, local_experts * capacity, column_count
    )
    returned = lax.all_to_all(expert_out, "ep", split_axis=0, concat_axis=0, tiled=True)
    picked = returned.reshape(expert_count * capacity, column_count)[targets].astype(jnp.float32)
    weighted = picked.reshape(token_rows, topk_count, column_count) * route_weights[:, :, None]
    combined = jnp.sum(weighted, axis=1) + shared_sum
    mixer_total, mixer_square, expert_total, expert_square = lax.psum(
        (
            jnp.sum(mixed, axis=1),
            jnp.sum(mixed * mixed, axis=1),
            jnp.sum(combined, axis=1),
            jnp.sum(combined * combined, axis=1),
        ),
        "tp",
    )
    full_width = column_count * tp_count
    out_mixer = finish(mixed, mixer_total, mixer_square, full_width, gain_mixer, bias_mixer)
    out_experts = finish(
        combined, expert_total, expert_square, full_width, gain_experts, bias_experts
    )
    return (out_mixer, out_experts)


PLANE = 2
SMALL_BYTES = 4 * 1024 * 1024
CORES = 2
VMEM_BYTES = 48 * 1024 * 1024


(
    UP,
    DOWN,
    ROUTE,
    PAIR,
    EDGE,
    CROSS,
    HIDDEN,
    SHARED,
    MIXER,
    PART,
    RETURN,
    STATS,
    ONWARD,
    ROUTE_UP,
    ROUTE_DOWN,
) = range(15)
LINE = 4
ALL, INNER, OUTER = range(3)


def plan(act):
    return [
        (ALL, act.shared, ()),
        (ALL, act.up, (0,)),
        (ALL, act.start_y, (0,)),
        (ALL, act.start_x, (0, 0)),
        (ALL, act.line, (1, 0, True)),
        (INNER, act.line, (2, 0)),
        (ALL, act.start_x, (0, 1)),
        (ALL, act.line, (1, 1, True)),
        (INNER, act.line, (2, 1)),
        (ALL, act.shared_relay, ()),
        (OUTER, act.line, (2, 0, True)),
        (INNER, act.line, (2, 2)),
        (INNER, act.line, (3, 0)),
        (ALL, act.cross, (1, 2)),
        (ALL, act.cross, (1, 3)),
        (INNER, act.line, (2, 3)),
        (OUTER, act.line, (2, 1, True)),
        (INNER, act.line, (3, 1)),
        (ALL, act.up, (1,)),
        (ALL, act.start, (1,)),
        (INNER, act.line, (3, 2)),
        (OUTER, act.line, (3, 0)),
        (OUTER, act.cross, (2, 2)),
        (OUTER, act.cross, (2, 3)),
        (OUTER, act.line, (3, 1)),
        (OUTER, act.relay, (0,)),
        (ALL, act.up, (2,)),
        (ALL, act.start, (2,)),
        (INNER, act.line, (3, 3)),
        (ALL, act.shared_dot, ()),
        (OUTER, act.line, (3, 2)),
        (OUTER, act.line, (3, 3)),
        (INNER, act.relay, (1,)),
        (ALL, act.up_part, (3, 0)),
        (ALL, act.start_part, (3, 0)),
        (INNER, act.relay, (2,)),
        (ALL, act.up_part, (3, 1)),
        (ALL, act.start_part, (3, 1)),
        (INNER, act.down, (1,)),
        (INNER, act.give_back, (1,)),
        (ALL, act.relay_part, (3, 0)),
        (INNER, act.down, (2,)),
        (ALL, act.relay_part, (3, 1)),
        (INNER, act.give_back, (2,)),
        (OUTER, act.relay, (2,)),
        (OUTER, act.relay, (1,)),
        (ALL, act.mixer, ()),
        (INNER, act.relay, (0,)),
        (ALL, act.down_part, (3, 0)),
        (ALL, act.give_back_part, (3, 0)),
        (ALL, act.down_part, (3, 1)),
        (ALL, act.give_back_part, (3, 1)),
        (OUTER, act.down, (2,)),
        (OUTER, act.down, (1,)),
        (OUTER, act.give_back, (2,)),
        (ALL, act.mixer_relay, (0,)),
        (OUTER, act.give_back, (1,)),
        (ALL, act.mixer_relay, (1,)),
        (ALL, act.down, (0,)),
        (ALL, act.give_back, (0,)),
        (ALL, act.mixer_dot, ()),
        (ALL, act.collect, (1,)),
        (ALL, act.collect, (2,)),
        (ALL, act.collect, (3,)),
    ]


def nearest_first(chips):
    def key(z):
        return lambda k: (abs(k - z), abs(2 * k - (chips - 1)))

    return [sorted((k for k in range(chips) if k != z), key=key(z)) for z in range(chips)]


def silu(value):
    return value / (1.0 + jnp.exp(-value))


def fused_kernel(
    shape,
    outer_hbm,
    inner_hbm,
    value_hbm,
    taps_hbm,
    mix_hbm,
    gain_m_hbm,
    bias_m_hbm,
    moe_hbm,
    ids_hbm,
    route_w_hbm,
    gate_hbm,
    up_hbm,
    down_hbm,
    shared_gate_hbm,
    shared_up_hbm,
    shared_down_hbm,
    gain_e_hbm,
    bias_e_hbm,
    out_m_ref,
    out_e_ref,
    outer_ref,
    inner_ref,
    value_ref,
    taps_ref,
    ids_ref,
    route_w_ref,
    gain_m_ref,
    bias_m_ref,
    gain_e_ref,
    bias_e_ref,
    mix_v,
    gate_v,
    up_v,
    down_v,
    shared_gate_v,
    shared_up_v,
    shared_down_v,
    tokens,
    route,
    rows_in,
    hidden,
    weighted,
    shared_hidden,
    border,
    edge,
    extended,
    peer_part,
    own_part,
    sent_sum,
    returned,
    stats_out,
    stats_in,
    mixed_ref,
    total_ref,
    load_sem,
    send_sem,
    recv_sem,
    line_recv,
    route_recv,
    return_recv,
):
    ep_count, tp_count, capacity, seq_length = shape
    chips = ep_count // CORES
    rows, cols = outer_ref.shape
    full_width = cols * tp_count
    me = lax.axis_index("ep")
    j = lax.axis_index("tp")
    z = me // CORES
    c = me % CORES
    x = j % PLANE
    y = j // PLANE
    jx = y * PLANE + (1 - x)
    jy = (1 - y) * PLANE + x
    jd = (1 - y) * PLANE + (1 - x)
    other = z * CORES + (1 - c)
    f32, bf16 = jnp.float32, jnp.bfloat16

    orders = nearest_first(chips)

    def pick(values):
        chosen = jnp.int32(values[0])
        for k in range(1, chips):
            chosen = jnp.where(z == k, values[k], chosen)
        return chosen

    sources = [z] + [pick([orders[k][s - 1] for k in range(chips)]) for s in range(1, chips)]

    def whole(k, q):
        s = orders[k].index(q) + 1
        return s == chips - 1 or s == chips - 2 and 0 < k < chips - 1

    def onward_of(k, s):
        q = orders[k][s - 1]
        n = k + 1 if q < k else k - 1
        there = 0 <= n < chips
        return n if there else k, there, there and whole(n, q)

    rising = pick([int(k + 1 < chips and whole(k + 1, k)) for k in range(chips)]) > 0
    falling = pick([int(k > 0 and whole(k - 1, k)) for k in range(chips)]) > 0

    loads = []

    def load(source, target):
        loads.append(pltpu.make_async_copy(source, target, load_sem.at[len(loads)]))
        loads[-1].start()
        return loads[-1]

    above = (z + 1) % chips
    below = (z + chips - 1) % chips
    higher = z + 1 < chips
    lower = z > 0
    beside = jnp.where(c > 0, me + 1, me + ep_count - 1) % ep_count
    slanted = jnp.where(c > 0, z + 1 < chips, z > 0)

    barrier = pltpu.get_barrier_semaphore()

    def greet(row, column):
        pl.semaphore_signal(
            barrier, inc=1, device_id=(row, column), device_id_type=pl.DeviceIdType.MESH
        )

    greet(other, j)
    greet(me, jx)
    greet(me, jy)
    pl.when(higher)(lambda: greet(above * CORES + c, j))
    pl.when(lower)(lambda: greet(below * CORES + c, j))
    pl.when(slanted)(lambda: greet(beside, j))
    greeted = 3 + higher.astype(jnp.int32) + lower.astype(jnp.int32) + slanted.astype(jnp.int32)

    moe_load = load(moe_hbm, tokens.at[z, 0])
    ids_load = load(ids_hbm, ids_ref)
    route_w_load = load(route_w_hbm, route_w_ref)
    inner_load = load(inner_hbm, inner_ref)
    value_load = load(value_hbm, value_ref)
    shared_gate_load = load(shared_gate_hbm, shared_gate_v)
    shared_up_load = load(shared_up_hbm, shared_up_v)
    gate_load = load(gate_hbm.at[0], gate_v)
    up_load = load(up_hbm.at[0], up_v)
    outer_load = load(outer_hbm, outer_ref)
    taps_load = load(taps_hbm, taps_ref)
    gain_m_load = load(gain_m_hbm, gain_m_ref)
    bias_m_load = load(bias_m_hbm, bias_m_ref)
    gain_e_load = load(gain_e_hbm, gain_e_ref)
    bias_e_load = load(bias_e_hbm, bias_e_ref)
    shared_down_load = load(shared_down_hbm, shared_down_v)
    down_load = load(down_hbm.at[0], down_v)
    mix_load = load(mix_hbm, mix_v)

    def loaded(*several):
        for one in several:
            one.wait()

    loaded(moe_load)
    with jax.named_scope("barrier"):
        pl.semaphore_wait(barrier, greeted)

    groups = {}
    numbers = {}

    def remote(source, target, sent, received, device):
        return pltpu.make_async_remote_copy(
            src_ref=source,
            dst_ref=target,
            send_sem=sent,
            recv_sem=received,
            device_id=device,
            device_id_type=pl.DeviceIdType.MESH,
        )

    def group(name):
        return send_sem.at[groups.setdefault(name, len(groups))]

    def number(name):
        return recv_sem.at[numbers.setdefault(name, len(numbers))]

    def send(many, name, source, target, device, received=None, when=None):
        copy = remote(source, target, group(many), number(name) if received is None else received, device)
        if when is None:
            copy.start()
        else:
            pl.when(when)(copy.start)

    def arrive(name, target, received=None):
        remote(target, target, group(EDGE), number(name) if received is None else received, (other, j)).wait_recv()

    def sent(many, ref, when=None):
        def wait():
            remote(ref, ref, group(many), number(EDGE), (other, j)).wait_send()

        if when is None:
            wait()
        else:
            pl.when(when)(wait)

    def columns(owner):
        return pl.ds(pl.multiple_of(owner * cols, cols), cols)

    def gather_x(name, ref):
        part = ref.at[:, columns(j)]
        send(name[0], name + (0,), part, part, (me, jx))

    def gather_y(name, ref):
        part = ref.at[:, columns(j)]
        send(name[0], name + (1,), part, part, (me, jy))

    def relay_x(name, ref):
        half = ref.shape[0] // 2
        arrive(name + (0,), ref.at[:, columns(jx)])
        part = ref.at[pl.ds(0, half), columns(jx)]
        send(name[0], name + (2,), part, part, (me, jy))

    def relay_y(name, ref):
        half = ref.shape[0] // 2
        arrive(name + (1,), ref.at[:, columns(jy)])
        part = ref.at[pl.ds(half, half), columns(jy)]
        send(name[0], name + (2,), part, part, (me, jx))

    def gather_finish(name, ref):
        arrive(name + (2,), ref.at[:, columns(jd)])

    quarters = (x, PLANE + y, 1 - x, PLANE + 1 - y)
    def line_start(k):
        part = tokens.at[z, 0, :, columns(quarters[k])]
        received = line_recv.at[z, k]
        more = k - k % PLANE
        device = (above * CORES + c, j)
        send((UP, more), (), part, part, device, received, rising if more else higher)
        device = (below * CORES + c, j)
        send((DOWN, more), (), part, part, device, received, falling if more else lower)

    line_start(0)
    send(PAIR, (PAIR, 0), tokens.at[z, 0], tokens.at[z, 1], (other, j))
    loaded(ids_load, route_w_load)
    named = lax.broadcasted_iota(jnp.int32, (ep_count, rows), 0)
    dense = jnp.zeros((ep_count, rows), f32)
    for k in range(ids_ref.shape[0]):
        dense = dense + jnp.where(named == ids_ref[k : k + 1, :], route_w_ref[k : k + 1, :], 0.0)
    route[z, 0] = dense
    own = route.at[z, 0]
    send(ROUTE_UP, (), own, own, (above * CORES + c, j), route_recv.at[z], higher)
    send(ROUTE_DOWN, (), own, own, (below * CORES + c, j), route_recv.at[z], lower)
    send(ROUTE, (ROUTE, 0), own, route.at[z, 1], (other, j))
    line_start(1)
    line_start(2)
    line_start(3)
    loaded(inner_load, value_load)
    product = (inner_ref[...].astype(f32) * value_ref[...].astype(f32)).astype(bf16)
    edge_rows = edge.shape[0]
    edge[...] = product[rows - edge_rows :]

    @pl.when(me == 0)
    def _():
        border[...] = jnp.zeros_like(border)

    pad = extended.shape[0] - rows
    extended[pad:, :] = product.astype(f32)
    last = me == ep_count - 1
    send(EDGE, EDGE, edge, border, ((me + 1) % ep_count, j), None, ~last)

    def dot(a, b):
        return jnp.dot(a, b, preferred_element_type=f32)

    def choice(s, p):
        weight = route[sources[s], p, pl.ds(me, 1), :]
        routed = (weight > 0.0).astype(f32)
        earlier = lax.broadcasted_iota(jnp.int32, (rows, rows), 0)
        later = lax.broadcasted_iota(jnp.int32, (rows, rows), 1)
        upper = (earlier <= later).astype(f32).astype(bf16)
        many = jnp.broadcast_to(routed, (16, rows)).astype(bf16)
        rank = dot(many, upper)[0:1, :] * routed
        slot = lax.broadcasted_iota(jnp.int32, (capacity, rows), 0).astype(f32) + 1.0
        return (slot == rank).astype(f32), weight

    def line_arrival(s, k, swap=False):
        q = sources[s]
        quarter = quarters[k]
        part = tokens.at[q, 0, :, columns(quarter)]
        if k == 1:
            own = route.at[q, 0]
            arrive((), own, route_recv.at[q])
            if (s, k) in onwards:
                onward, more = onwards[s, k]
                device = (onward * CORES + c, j)
                send((ROUTE, s), (), own, own, device, route_recv.at[q], more)
            send(ROUTE, (ROUTE, s), own, route.at[q, 1], (other, j))
        arrive((), part, line_recv.at[q, k])
        onward_send(s, k)
        if swap:
            send((CROSS, s), (CROSS, s, k), part, part, (me, (jx, jy)[k]))
        send(PAIR, (PAIR, s), part, tokens.at[q, 1, :, columns(quarter)], (other, j))

    onwards = {}
    for s in range(1, chips):
        for k in range(tp_count):
            told = [onward_of(n, s)[1 if k < PLANE else 2] for n in range(chips)]
            if any(told):
                onward = pick([onward_of(n, s)[0] for n in range(chips)])
                onwards[s, k] = (onward, pick([int(t) for t in told]) > 0)

    def onward_send(s, k):
        q = sources[s]
        part = tokens.at[q, 0, :, columns(quarters[k])]
        if (s, k) in onwards:
            onward, more = onwards[s, k]
            device = (onward * CORES + c, j)
            send((ONWARD, s, k - k % PLANE), (), part, part, device, line_recv.at[q, k], more)

    def cross_arrival(s, k):
        q = sources[s]
        part = tokens.at[q, 0, :, columns(quarters[k])]
        arrive((CROSS, s, k - PLANE), part)
        onward_send(s, k)
        send(PAIR, (PAIR, s), part, tokens.at[q, 1, :, columns(quarters[k])], (other, j))

    def expert_up(s):
        q = sources[s]
        arrive((ROUTE, s), route.at[q, 1])
        if s == 0:
            loaded(gate_load, up_load)
        chosen = [choice(s, p)[0] for p in range(CORES)]
        for p, picks in enumerate(chosen):
            if p == 1:
                arrive((PAIR, s), tokens.at[q, 1])
            rows_in[p * capacity : (p + 1) * capacity, :] = dot(
                picks.astype(bf16), tokens[q, p]
            ).astype(bf16)
        held = silu(dot(rows_in[...], gate_v[...])) * dot(rows_in[...], up_v[...])
        hidden[q, :, columns(j)] = held.astype(bf16)

    def up_part(s, t):
        q = sources[s]
        p = (t + c) % CORES
        if t == 0:
            arrive((ROUTE, s), route.at[q, 1])
        picks, _ = choice(s, p)
        if t == 0:
            arrive((PAIR, s), tokens.at[q, 1])
        taken = dot(picks.astype(bf16), tokens[q, p]).astype(bf16)
        held = silu(dot(taken, gate_v[...])) * dot(taken, up_v[...])
        hidden[q, t * capacity : (t + 1) * capacity, columns(j)] = held.astype(bf16)

    def part_ref(s, t):
        return hidden.at[sources[s], pl.ds(t * capacity, capacity)]

    def down_part(s, t):
        q = sources[s]
        picks, weight = choice(s, (t + c) % CORES)
        gather_finish((HIDDEN, s, t), part_ref(s, t))
        full = dot(hidden[q, t * capacity : (t + 1) * capacity], down_v[...])
        scale = jnp.sum(picks * weight, axis=1, keepdims=True)
        scaled = (full * scale).astype(bf16)
        spread = lax.dot_general(
            picks.astype(bf16), scaled, (((0,), (0,)), ((), ())), preferred_element_type=f32
        ).astype(bf16)

        @pl.when(c == t)
        def _():
            sent_sum[q] = spread

        @pl.when(c != t)
        def _():
            own_part[q] = spread
            send(PART, (PART, s), own_part.at[q], peer_part.at[q], (other, j))

    def return_part(s, t):
        @pl.when(c == t)
        def _():
            expert_return(s)

    def start_x(s, t=None):
        ref = hidden.at[sources[s]] if t is None else part_ref(s, t)
        gather_x((HIDDEN, s), ref)

    def start_y(s):
        gather_y((HIDDEN, s), hidden.at[sources[s]])

    def start(s):
        start_x(s)
        start_y(s)

    def relay(s):
        relay_x((HIDDEN, s), hidden.at[sources[s]])
        relay_y((HIDDEN, s), hidden.at[sources[s]])

    def start_part(s, t):
        gather_x((HIDDEN, s, t), part_ref(s, t))
        gather_y((HIDDEN, s, t), part_ref(s, t))

    def relay_part(s, t):
        relay_x((HIDDEN, s, t), part_ref(s, t))
        relay_y((HIDDEN, s, t), part_ref(s, t))

    def collect(s):
        q = sources[s]
        arrive((), returned.at[q], return_recv.at[q])
        total_ref[...] = total_ref[...] + returned[q].astype(f32)

    def expert_down(s):
        q = sources[s]
        gather_finish((HIDDEN, s), hidden.at[q])
        full = dot(hidden[q], down_v[...])
        for p in reversed(range(CORES)):
            picks, weight = choice(s, p)
            scale = jnp.sum(picks * weight, axis=1, keepdims=True)
            scaled = (full[p * capacity : (p + 1) * capacity] * scale).astype(bf16)
            spread = lax.dot_general(
                picks.astype(bf16), scaled, (((0,), (0,)), ((), ())), preferred_element_type=f32
            )
            if p == 1:
                own_part[q] = spread.astype(bf16)
                send(PART, (PART, s), own_part.at[q], peer_part.at[q], (other, j))
            elif s == 0:
                total_ref[...] = total_ref[...] + spread
            else:
                sent_sum[q] = spread.astype(bf16)

    def expert_return(s):
        q = sources[s]
        arrive((PART, s), peer_part.at[q])
        if s == 0:
            total_ref[...] = total_ref[...] + peer_part[q].astype(f32)
        else:
            sent_sum[q] = (sent_sum[q].astype(f32) + peer_part[q].astype(f32)).astype(bf16)
            send(RETURN, (), sent_sum.at[q], returned.at[z], (q * CORES + c, j), return_recv.at[z])

    def stats_start(k, values):
        lane = lax.broadcasted_iota(jnp.int32, (rows, rows), 1)
        total = jnp.sum(values, axis=1, keepdims=True)
        square = jnp.sum(values * values, axis=1, keepdims=True)
        tile = jnp.where(lane == 0, total, jnp.where(lane == 1, square, 0.0))
        stats_out[k] = tile.T[0 : stats_out.shape[1], :]
        for n, peer in enumerate((jx, jy, jd)):
            send((STATS, k), (STATS, k), stats_out.at[k], stats_in.at[k, n], (me, peer))

    def stats_finish(k, values, gain_ref, bias_ref, out_ref):
        tile = stats_out[k]
        arrive((STATS, k), stats_in.at[k])
        for n in range(tp_count - 1):
            tile = tile + stats_in[k, n]
        padded = jnp.concatenate(
            [tile, jnp.zeros((rows - tile.shape[0], rows), f32)], axis=0
        ).T
        average = padded[:, 0:1] / full_width
        spread = padded[:, 1:2] / full_width - average * average
        scaled = (values - average) * lax.rsqrt(spread + 1e-05)
        out_ref[...] = (
            scaled * gain_ref[...].astype(f32).reshape(1, cols)
            + bias_ref[...].astype(f32).reshape(1, cols)
        ).astype(bf16)

    def shared_start():
        loaded(shared_gate_load, shared_up_load)
        own = tokens[z, 0]
        held = silu(dot(own, shared_gate_v[...])) * dot(own, shared_up_v[...])
        shared_hidden[:, columns(j)] = held.astype(bf16)
        gather_x((SHARED,), shared_hidden)
        gather_y((SHARED,), shared_hidden)

    def mixer_ref(t):
        return weighted.at[pl.ds(t * (rows // 2), rows // 2)]

    def mixer_start():
        pl.when(me > 0)(lambda: arrive(EDGE, border))
        loaded(outer_load, taps_load)
        extended[pad - edge_rows : pad, :] = border[...].astype(f32)
        places = (me * rows + lax.broadcasted_iota(jnp.int32, (rows, 1), 0)) % seq_length
        taps_count = taps_ref.shape[0]
        convolved = jnp.zeros((rows, cols), f32)
        for offset in range(taps_count):
            delay = taps_count - 1 - offset
            delayed = extended[pad - delay : pad - delay + rows, :]
            kept = (places >= delay).astype(f32)
            convolved = convolved + taps_ref[offset : offset + 1, :].astype(f32) * delayed * kept
        weighted[:, columns(j)] = (outer_ref[...].astype(f32) * convolved).astype(bf16)
        for t in range(2):
            gather_x((MIXER, t), mixer_ref(t))
            gather_y((MIXER, t), mixer_ref(t))

    def shared_relay():
        relay_x((SHARED,), shared_hidden)
        relay_y((SHARED,), shared_hidden)

    def mixer_relay(t):
        relay_x((MIXER, t), mixer_ref(t))
        relay_y((MIXER, t), mixer_ref(t))

    def mixer_dot():
        gather_finish((MIXER, 0), mixer_ref(0))
        gather_finish((MIXER, 1), mixer_ref(1))
        loaded(mix_load)
        mixed_ref[...] = dot(weighted[...], mix_v[...])
        stats_start(0, mixed_ref[...])

    def mixer_end():
        loaded(gain_m_load, bias_m_load, gain_e_load, bias_e_load)
        stats_finish(0, mixed_ref[...], gain_m_ref, bias_m_ref, out_m_ref)

    def shared_dot():
        gather_finish((SHARED,), shared_hidden)
        loaded(shared_down_load, down_load)
        total_ref[...] = dot(shared_hidden[...], shared_down_v[...])

    act = types.SimpleNamespace(
        shared=shared_start,
        up=expert_up,
        start=start,
        start_x=start_x,
        start_y=start_y,
        line=line_arrival,
        cross=cross_arrival,
        relay=relay,
        down=expert_down,
        give_back=expert_return,
        up_part=up_part,
        start_part=start_part,
        relay_part=relay_part,
        down_part=down_part,
        give_back_part=return_part,
        shared_relay=shared_relay,
        shared_dot=shared_dot,
        mixer=mixer_start,
        mixer_relay=mixer_relay,
        mixer_dot=mixer_dot,
        collect=collect,
    )
    inner = (z > 0) & (z < chips - 1)
    for where, step, which in plan(act):
        if where == ALL:
            step(*which)
        else:
            pl.when(inner if where == INNER else ~inner)(functools.partial(step, *which))
    with jax.named_scope("stats"):
        stats_start(1, total_ref[...])
    with jax.named_scope("mixer_end"):
        mixer_end()
    with jax.named_scope("drain"):
        lines = tokens.at[0, 0, :, pl.ds(0, PLANE * cols)]
        sent((UP, 0), lines, higher)
        sent((DOWN, 0), lines, lower)
        sent((UP, PLANE), lines, rising)
        sent((DOWN, PLANE), lines, falling)
        for s, k in onwards:
            if k % PLANE == 0:
                sent((ONWARD, s, k), lines, onwards[s, k][1])
            if k == 0:
                sent((ROUTE, s), route.at[0, 0], onwards[s, k][1])
        sent(ROUTE_UP, route.at[0, 0], higher)
        sent(ROUTE_DOWN, route.at[0, 0], lower)
        sent(PAIR, tokens.at[:, 0])
        sent(ROUTE, route.at[:, 0])
        sent(EDGE, edge, ~last)
        sent((CROSS, 1), lines)
        sent((CROSS, 2), lines, ~inner)
        gathered = pl.ds(0, (tp_count - 1) * cols)
        sent(HIDDEN, hidden.at[:, :, gathered])
        sent(SHARED, shared_hidden.at[:, gathered])
        sent(MIXER, weighted.at[:, gathered])
        sent(PART, own_part)
        sent(RETURN, own_part.at[pl.ds(0, chips - 1)])
        sent((STATS, 0), stats_in.at[0])
    with jax.named_scope("finish"):
        stats_finish(1, total_ref[...], gain_e_ref, bias_e_ref, out_e_ref)
    with jax.named_scope("sent"):
        sent((STATS, 1), stats_in.at[1])


def pass_kernel(first_ref, second_ref, out_first_ref, out_second_ref):
    out_first_ref[...] = first_ref[...]
    out_second_ref[...] = second_ref[...]


def fused_device(
    outer_gate,
    inner_gate,
    conv_value,
    conv_taps,
    mix_out,
    gain_mixer,
    bias_mixer,
    moe_input,
    route_ids,
    route_weights,
    expert_gate,
    expert_up,
    expert_down,
    shared_gate,
    shared_up,
    shared_down,
    gain_experts,
    bias_experts,
):
    rows, cols = outer_gate.shape
    width = moe_input.shape[1]
    ep_count = lax.axis_size("ep")
    tp_count = lax.axis_size("tp")
    chips = ep_count // CORES
    capacity = max(2, 3 * rows * route_ids.shape[1] // (2 * ep_count))
    seq_length = rows * ep_count // SEQS
    bf16, f32 = jnp.bfloat16, jnp.float32
    vmem = pl.BlockSpec(memory_space=pltpu.VMEM)
    hbm = pl.BlockSpec(memory_space=pl.ANY)
    copies = 5 * chips + 23
    weight = pltpu.VMEM((width, cols), bf16)
    scratch = [
        *([pltpu.VMEM((rows, cols), bf16)] * 3),
        pltpu.VMEM(conv_taps.shape, bf16),
        pltpu.VMEM(route_ids.shape[::-1], jnp.int32),
        pltpu.VMEM(route_weights.shape[::-1], f32),
        *([pltpu.VMEM((cols,), bf16)] * 4),
        *([weight] * 7),
        pltpu.VMEM((chips, CORES, rows, width), bf16),
        pltpu.VMEM((chips, CORES, ep_count, rows), f32),
        pltpu.VMEM((CORES * capacity, width), bf16),
        pltpu.VMEM((chips, CORES * capacity, width), bf16),
        pltpu.VMEM((rows, width), bf16),
        pltpu.VMEM((rows, width), bf16),
        pltpu.VMEM((16, cols), bf16),
        pltpu.VMEM((16, cols), bf16),
        pltpu.VMEM((rows + 16, cols), f32),
        pltpu.VMEM((chips, rows, cols), bf16),
        pltpu.VMEM((chips, rows, cols), bf16),
        pltpu.VMEM((chips, rows, cols), bf16),
        pltpu.VMEM((chips, rows, cols), bf16),
        pltpu.VMEM((2, 8, rows), f32),
        pltpu.VMEM((2, tp_count - 1, 8, rows), f32),
        pltpu.VMEM((rows, cols), f32),
        pltpu.VMEM((rows, cols), f32),
        pltpu.SemaphoreType.DMA((18,)),
        pltpu.SemaphoreType.DMA((chips + 22,)),
        pltpu.SemaphoreType.DMA((copies,)),
        pltpu.SemaphoreType.DMA((chips, tp_count)),
        pltpu.SemaphoreType.DMA((chips,)),
        pltpu.SemaphoreType.DMA((chips,)),
    ]
    out = jax.ShapeDtypeStruct((rows, cols), bf16)
    near = pltpu.VMEM((rows, cols), bf16)
    given = (
        outer_gate,
        inner_gate,
        conv_value,
        conv_taps,
        mix_out,
        gain_mixer,
        bias_mixer,
        moe_input,
        route_ids.T,
        route_weights.T,
        expert_gate,
        expert_up,
        expert_down,
        shared_gate,
        shared_up,
        shared_down,
        gain_experts,
        bias_experts,
    )
    first, second = pl.pallas_call(
        functools.partial(fused_kernel, (ep_count, tp_count, capacity, seq_length)),
        out_shape=(near, near),
        in_specs=[hbm] * 18,
        out_specs=(vmem, vmem),
        scratch_shapes=scratch,
        compiler_params=pltpu.CompilerParams(
            collective_id=0, has_side_effects=True, vmem_limit_bytes=VMEM_BYTES
        ),
    )(*(pltpu.with_memory_space_constraint(one, pltpu.HBM) for one in given))
    return pl.pallas_call(
        pass_kernel,
        out_shape=(out, out),
        in_specs=[vmem, vmem],
        out_specs=(vmem, vmem),
        compiler_params=pltpu.CompilerParams(vmem_limit_bytes=SMALL_BYTES),

    )(first, second)


def on_device(*arrays):
    local_experts = arrays[10].shape[0]
    square = lax.axis_size("tp") == PLANE * PLANE
    if square and local_experts == 1 and lax.axis_size("ep") == CORES * LINE:
        return fused_device(*arrays)
    return plain_device(*arrays)


def solution(mesh):
    in_specs = (
        P("ep", "tp"),
        P("ep", "tp"),
        P("ep", "tp"),
        P(None, "tp"),
        P(None, "tp"),
        P("tp"),
        P("tp"),
        P("ep", None),
        P("ep", None),
        P("ep", None),
        P("ep", None, "tp"),
        P("ep", None, "tp"),
        P("ep", None, "tp"),
        P(None, "tp"),
        P(None, "tp"),
        P(None, "tp"),
        P("tp"),
        P("tp"),
    )
    out_specs = (P("ep", "tp"), P("ep", "tp"))
    return jax.shard_map(
        on_device, mesh=mesh, in_specs=in_specs, out_specs=out_specs, check_vma=False
    )
```
